32 devices in a mesh: fs: 4 (over z), rep: 4 (over y, x), tp: 2 (over core).
Axes of the slice: x: 2, y: 2, z: 4, core: 2. Of those that a mesh axis runs over, the one named last changes fastest.
Arguments:
- first_mix: bfloat16 [12288, 2048], P(('fs', 'rep'), 'tp'), may hold values from -6 to 6
- second_mix: bfloat16 [12288, 2048], P(('fs', 'rep'), 'tp'), may hold values from -6 to 6
- lambda_head: float32 [8], P('tp'), may hold values from 0.3 to 0.8
- head_gain: float32 [256], replicated, may hold values from 0.1 to 1.9
- out_cotangent: bfloat16 [12288, 2048], P(('fs', 'rep')), may hold values from -0.053955078 to 0.053955078
- basis: bfloat16 [2048, 256], P('tp'), may hold values from -0.125 to 0.125
- weight: float32 [2048, 2048], P('tp', 'fs'), may hold values from -3 to 3
- first_moment: float32 [2048, 256], P('fs', 'tp'), may hold values from -4.5 to 4.5
- second_moment: float32 [2048, 256], P('fs', 'tp'), may hold values from 0.05 to 0.5
Outputs:
- weight_new: float32 [2048, 2048], P('tp', 'fs')
- weight_copy: bfloat16 [2048, 2048], P('tp')
- step_out: float32 [2048, 2048], P('tp', 'fs')
- first_new: float32 [2048, 256], P('fs', 'tp')
- second_new: float32 [2048, 256], P('fs', 'tp')
The draws below stay inside these ranges and needn't reach their ends.
All inputs are finite; a program needn't handle non-finite values.
Results may differ from the reference program's by a relative error of at most 0.0075.
Values may be sent and summed in bfloat16 or wider, within the bound.
A program may use at most 64 MiB of HBM per device.

```python
import math
import jax
import jax.numpy as jnp
from jax import lax

D = 2048
HEADS = 8
HEAD_V = 256
RANK = 256
TOK_DEV = 768
HV = 2048
TOKENS = 12288


def draw_first_moment(key, part):
    draw_base = jnp.clip(jax.random.normal(key, (D, RANK), jnp.float32), -3.0, 3.0)
    roughness = jax.random.uniform(jax.random.fold_in(key, 7), (D, RANK), jnp.float32, 0.5, 1.5)
    rising = 10.0 ** (jnp.arange(D, dtype=jnp.float32) / D)
    return draw_base * 0.1 * rising[:, None] * roughness


def raised(entries, own_key, source, target, parts, factor):
    def block_of(axis_at):
        return (jnp.arange(entries.shape[axis_at]) // (entries.shape[axis_at] // parts)).reshape((-1,) + (1,) * (entries.ndim - 1 - axis_at))

    near = jax.random.permutation(own_key, parts)[block_of(target)]
    second = (block_of(target) + parts // 2) % parts
    return jnp.where((block_of(source) == near) | (block_of(source) == second), factor * entries, entries)


def shard_levels(stream_key, extent, cuts, low, largest):
    def one(axis_at, blocks):
        steps = jax.random.uniform(jax.random.fold_in(jax.random.fold_in(stream_key, 6), axis_at), (blocks,), jnp.float32, low / len(cuts), largest / len(cuts))
        return jnp.repeat(jnp.exp(steps), extent[axis_at] // blocks).reshape((-1,) + (1,) * (len(extent) - axis_at - 1))

    gain = one(*cuts[0])
    for cut in cuts[1:]:
        gain = gain * one(*cut)
    return gain


def bell_draw(stream_key, shape, deviation, limit, cuts=(), kind=jnp.bfloat16):
    loudness = shard_levels(stream_key, shape, cuts, -0.22, 0.18) if cuts else 1.0
    array = jax.random.normal(stream_key, shape, jnp.float32) * deviation * loudness
    return jnp.minimum(jnp.maximum(array, -limit), limit).astype(kind)


def gaussian_with(key, extent, width, most, cuts, heavy, held_as=jnp.bfloat16):
    values = width * jax.random.normal(key, extent, jnp.float32)
    if cuts:
        values = values * shard_levels(key, extent, cuts, -0.22, 0.18)
    return jnp.clip(raised(values, jax.random.fold_in(key, 3), *heavy), -most, most).astype(held_as)


def setup_inputs(seed: int = 0) -> dict:
    splits = jax.random.split(jax.random.key(seed), 10)
    return {
        "first_mix": bell_draw(splits[0], (TOKENS, HV), 1.0, 6.0, ((0, 16), (1, 2))),
        "second_mix": bell_draw(splits[1], (TOKENS, HV), 1.0, 6.0, ((0, 16), (1, 2))),
        "lambda_head": jnp.clip(0.3 + 0.5 * jax.random.uniform(splits[2], (HEADS,), jnp.float32) ** shard_levels(splits[2], (HEADS,), ((0, 2),), -0.2, 0.2), 0.3, 0.8),
        "head_gain": jnp.clip(1.0 + 0.18 * jax.random.normal(splits[3], (HEAD_V,), jnp.float32), 0.1, 1.9),
        "out_cotangent": gaussian_with(splits[4], (TOKENS, D), (TOKENS ** -0.5), 0.053955078, ((0, 16),), (0, 1, 16, 2.0)),
        "basis": bell_draw(splits[5], (HV, RANK), HV ** -0.5, 0.125, ((0, 2),)),
        "weight": bell_draw(splits[6], (HV, D), 0.5, 3.0, ((0, 2), (1, 4)), jnp.float32),
        "first_moment": draw_first_moment(jax.random.fold_in(splits[9], 71), 0),
        "second_moment": jnp.clip(jnp.exp(math.log(0.5) - 2.3025851 * jax.random.uniform(splits[8], (D, RANK), jnp.float32) ** shard_levels(splits[8], (D, RANK), ((0, 4), (1, 2)), -0.2, 0.2)), 0.05, 0.5),
    }


out_scale = 0.8
beta_first = 0.9
beta_second = 0.95

def head_output(first_piece, second_piece, lambdas, head_gain):
    token_count = first_piece.shape[0]
    head_width = head_gain.shape[0]
    head_count = lambdas.shape[0] // head_width
    mixture = first_piece.astype(jnp.float32) - lambdas[None, :] * second_piece.astype(jnp.float32)
    grouped = mixture.reshape(token_count, head_count, head_width)
    inverse = lax.rsqrt(lax.optimization_barrier(jnp.mean(grouped * grouped, axis=-1, keepdims=True)) + 1e-06)
    normed = grouped * inverse * head_gain[None, None, :] * out_scale
    return normed.reshape(token_count, head_count * head_width).astype(jnp.bfloat16)

def reference(first_mix, second_mix, lambda_head, head_gain, out_cotangent, basis, weight, first_moment, second_moment):
    block_count = first_mix.shape[0] // TOK_DEV
    lambdas = jnp.repeat(lambda_head, HEAD_V)

    def accumulate(running, pieces):
        first_piece, second_piece, cot_piece = pieces
        head_out = head_output(first_piece, second_piece, lambdas, head_gain)
        term = lax.dot_general(cot_piece, head_out, (((0,), (0,)), ((), ())), preferred_element_type=jnp.float32)
        return (running + term, None)
    grad_t, _ = lax.scan(accumulate, jnp.zeros((D, HV), jnp.float32), (first_mix.reshape(block_count, TOK_DEV, HV), second_mix.reshape(block_count, TOK_DEV, HV), out_cotangent.reshape(block_count, TOK_DEV, D)))
    basis_wide = basis.astype(jnp.float32)
    projected = jnp.dot(grad_t, basis_wide, precision=lax.Precision.HIGHEST)
    first_new = beta_first * first_moment + (1.0 - beta_first) * projected
    second_new = beta_second * second_moment + (1.0 - beta_second) * projected * projected
    direction = first_new / (jnp.sqrt(second_new) + 1e-08)
    spread = jnp.sqrt(jnp.mean(direction * direction))
    step_out = jnp.dot(basis_wide, direction.T, precision=lax.Precision.HIGHEST) * (-1.0 / (spread + 1e-06))
    weight_new = weight + step_out
    weight_copy = weight_new.astype(jnp.bfloat16)
    return (weight_new, weight_copy, step_out, first_new, second_new)
```

```python
import functools

import jax
import jax.numpy as jnp
from jax import lax
from jax.experimental import pallas as pl
from jax.experimental.pallas import tpu as pltpu
from jax.sharding import PartitionSpec as P

MESH = pl.DeviceIdType.MESH

vmem_grant = 67043328
out_scale = 0.8
beta_first = 0.9
beta_second = 0.95
quarter_chunks = 4
extra_part = 8


def head_output(first_piece, second_piece, lambdas, head_gain):
    token_count = first_piece.shape[0]
    head_width = head_gain.shape[0]
    head_count = lambdas.shape[0] // head_width
    mixture = first_piece.astype(jnp.float32) - lambdas[None, :] * second_piece.astype(jnp.float32)
    grouped = mixture.reshape(token_count, head_count, head_width)
    inverse = lax.rsqrt(jnp.mean(grouped * grouped, axis=-1, keepdims=True) + 1e-06)
    normed = grouped * inverse * head_gain[None, None, :] * out_scale
    return normed.reshape(token_count, head_count * head_width).astype(jnp.bfloat16)


def split_product(narrow, wide, numbers):
    upper = wide.astype(jnp.bfloat16)
    lower = (wide - upper.astype(jnp.float32)).astype(jnp.bfloat16)
    return lax.dot_general(
        narrow, upper, numbers, preferred_element_type=jnp.float32
    ) + lax.dot_general(narrow, lower, numbers, preferred_element_type=jnp.float32)


def body(
    first_mix,
    second_mix,
    lambda_head,
    head_gain,
    out_cotangent,
    basis,
    weight,
    first_moment,
    second_moment,
):
    lambdas = jnp.repeat(lambda_head, head_gain.shape[0])
    head_out = head_output(first_mix, second_mix, lambdas, head_gain)
    reduced = jnp.dot(head_out, basis, preferred_element_type=jnp.float32)
    proj_rows = lax.psum_scatter(
        split_product(out_cotangent, reduced, (((0,), (0,)), ((), ()))),
        "fs",
        scatter_dimension=0,
        tiled=True,
    )
    proj_rows = lax.psum_scatter(proj_rows, "tp", scatter_dimension=1, tiled=True)
    projected = lax.psum(proj_rows, "rep")
    first_new = beta_first * first_moment + (1.0 - beta_first) * projected
    second_new = beta_second * second_moment + (1.0 - beta_second) * projected * projected
    direction = first_new / (jnp.sqrt(second_new) + 1e-08)
    energy = lax.psum(jnp.sum(direction * direction), ("fs", "tp"))
    entries = direction.shape[0] * direction.shape[1] * lax.axis_size("fs") * lax.axis_size("tp")
    spread = jnp.sqrt(energy / entries)
    full_direction = lax.all_gather(direction, "tp", axis=1, tiled=True)
    step_out = split_product(basis, full_direction, (((1,), (1,)), ((), ()))) * (
        -1.0 / (spread + 1e-06)
    )
    weight_new = weight + step_out
    weight_copy = lax.all_gather(weight_new.astype(jnp.bfloat16), "fs", axis=1, tiled=True)
    return (weight_new, weight_copy, step_out, first_new, second_new)


def exchange_kernel(
    sizes,
    lambda_ref,
    gain_ref,
    first_hbm,
    second_hbm,
    cot_hbm,
    basis_hbm,
    weight_hbm,
    moment1_hbm,
    moment2_hbm,
    copy_ref,
    new_ref,
    step_ref,
    first_new_ref,
    second_new_ref,
    first_v,
    second_v,
    cot_v,
    basis_v,
    weight_v,
    gathered_v,
    moment1_v,
    moment2_v,
    half_mine_v,
    half_send_v,
    half_recv_v,
    turned_v,
    mine_v,
    plane_send_v,
    plane_recv_v,
    line_send_v,
    line_recv_v,
    projected_v,
    direction_v,
    joined_v,
    load_sem,
    tile_sem,
    wz_send,
    wf_send,
    wz_recv,
    wp_send,
    wp_recv,
    wr_send,
    wr_recv,
    half_send,
    half_recv,
    plane_send,
    plane_recv,
    line_send,
    line_recv,
    proj_send,
    proj_recv,
    dz_send,
    dz_recv,
    dp_send,
    dp_recv,
    dt_send,
    dt_recv,
):
    line, plane = sizes
    fs, rep, tp = lax.axis_index("fs"), lax.axis_index("rep"), lax.axis_index("tp")
    other = 1 - tp
    tokens, width = cot_v.shape
    half, quarter = direction_v.shape[-2:]
    values, shard = weight_v.shape
    quarter_rows = values // plane
    chunk = quarter_rows // quarter_chunks
    head_width = gain_ref.shape[1]
    heads = first_v.shape[1] // head_width
    tiles = tile_sem.shape[0]
    tile = tokens // tiles

    fast_side = rep + 1 - 2 * lax.rem(rep, 2)
    slow_side = lax.rem(rep + 2, 4)
    far_side = 3 - rep
    sides = (fast_side, slow_side)
    peers = (far_side, slow_side, fast_side, rep)

    near_source = 1 + lax.rem(fs, 2)
    last_source = jnp.where(fs < 2, 3, 0)
    sources = (near_source, 6 - fs - near_source - last_source, last_source)
    nexts = tuple(jnp.where(source < fs, fs + 1, fs - 1) for source in sources)
    goes_on = tuple((to >= 0) & (to < line) for to in nexts)

    def remote(source, target, send, recv, where):
        return pltpu.make_async_remote_copy(
            src_ref=source,
            dst_ref=target,
            send_sem=send,
            recv_sem=recv,
            device_id=where,
            device_id_type=MESH,
        )

    def rows_of(owner, start, size):
        return pl.ds(pl.multiple_of(owner * quarter_rows + start, 16), size)

    def weight_load(owner, at):
        rows = rows_of(owner, 0, quarter_rows)
        return pltpu.make_async_copy(weight_hbm.at[rows], weight_v.at[rows], load_sem.at[at])

    weight_loads = [weight_load(owner, at) for at, owner in enumerate((rep, far_side) + sides)]
    basis_loads = [
        pltpu.make_async_copy(
            basis_hbm.at[:, pl.ds(pl.multiple_of(side * half, half), half)],
            basis_v.at[:, pl.ds(at * half, half)],
            load_sem.at[4 + at],
        )
        for at, side in enumerate((tp, other))
    ]
    cot_load = pltpu.make_async_copy(cot_hbm, cot_v, load_sem.at[6])
    moment_loads = [
        pltpu.make_async_copy(moment1_hbm, moment1_v, load_sem.at[7]),
        pltpu.make_async_copy(moment2_hbm, moment2_v, load_sem.at[8]),
    ]
    weight_loads[0].start()
    for load in basis_loads:
        load.start()
    tile_loads = []
    for t in range(tiles):
        rows = pl.ds(t * tile, tile)
        pieces = (
            pltpu.make_async_copy(first_hbm.at[rows], first_v.at[rows], tile_sem.at[t, 0]),
            pltpu.make_async_copy(second_hbm.at[rows], second_v.at[rows], tile_sem.at[t, 1]),
        )
        for piece in pieces:
            piece.start()
        tile_loads.append(pieces)
    cot_load.start()
    weight_loads[1].start()
    for load in moment_loads + weight_loads[2:]:
        load.start()

    barrier = pltpu.get_barrier_semaphore()
    for step in range(1, line):
        pl.semaphore_signal(
            barrier, inc=1, device_id={"fs": lax.rem(fs + step, line)}, device_id_type=MESH
        )
    for step in range(plane - 1):
        pl.semaphore_signal(
            barrier, inc=1, device_id={"rep": peers[step]}, device_id_type=MESH
        )
    pl.semaphore_signal(barrier, inc=1, device_id={"tp": other}, device_id_type=MESH)
    pl.semaphore_wait(barrier, line + plane - 1)

    sends = []
    guarded = []

    extra = quarter_rows * extra_part // 16
    rest = (quarter_rows - extra) // 2
    pieces = [(rep, c * chunk, chunk) for c in range(quarter_chunks)]
    pieces += [(far_side, c * (extra // 2), extra // 2) for c in range(2)]
    quarters = tuple(range(quarter_chunks))
    extras = (quarter_chunks, quarter_chunks + 1)

    def line_copy(source, c, send, to):
        here = gathered_v.at[source, rows_of(*pieces[c])]
        return remote(here, here, send, wz_recv.at[source, c], {"fs": to})

    def start_if(wanted, copy):
        @pl.when(wanted)
        def _():
            copy.start()

        guarded.append((wanted, copy))

    def narrow(c):
        rows = rows_of(*pieces[c])
        gathered_v[fs, rows] = weight_v[rows].astype(jnp.bfloat16)

    def send_own(c):
        start_if(fs < line - 1, line_copy(fs, c, wz_send.at[0, c], fs + 1))
        start_if(fs > 0, line_copy(fs, c, wz_send.at[1, c], fs - 1))

    def arrive(t, c):
        copy = line_copy(sources[t], c, wf_send.at[t, c], nexts[t])
        copy.wait_recv()
        start_if(goes_on[t], copy)
        if c in quarters:
            here = gathered_v.at[sources[t], rows_of(*pieces[c])]
            for side in range(2):
                copy = remote(
                    here,
                    here,
                    wp_send.at[t, c, side],
                    wp_recv.at[t, c, side],
                    {"rep": sides[side]},
                )
                copy.start()
                sends.append(copy)

    waited = set()

    def from_side(t, c, side):
        if (t, c, side) not in waited:
            waited.add((t, c, side))
            here = gathered_v.at[sources[t], rows_of(sides[side], c * chunk, chunk)]
            remote(
                here,
                here,
                wp_send.at[t, c, side],
                wp_recv.at[t, c, side],
                {"rep": sides[side]},
            ).wait_recv()

    def relay_copy(t, side, owner):
        here = gathered_v.at[sources[t], rows_of(owner, extra + side * rest, rest)]
        return remote(
            here, here, wr_send.at[t, side], wr_recv.at[t, side], {"rep": sides[1 - side]}
        )

    def relay(t):
        for side in range(2):
            from_side(t, (extra + side * rest) // chunk, side)
            copy = relay_copy(t, side, sides[side])
            copy.start()
            sends.append(copy)

    def finish(t):
        for c in quarters:
            for side in range(2):
                from_side(t, c, side)
        for side in range(2):
            relay_copy(t, side, far_side).wait_recv()

    weight_loads[0].wait()
    for c in quarters:
        narrow(c)
        send_own(c)

    for load in basis_loads:
        load.wait()
    gain = gain_ref[...] * out_scale
    half_copies = []

    def join_pair(t):
        half_copies[t].wait_recv()
        both = half_mine_v[t] + half_recv_v[t]
        turned_v[:, t * tile : (t + 1) * tile] = both.T.astype(jnp.bfloat16)

    for t in range(tiles):
        for piece in tile_loads[t]:
            piece.wait()
        rows = pl.ds(t * tile, tile)
        reduced = None
        for h in range(heads):
            lanes = pl.ds(h * head_width, head_width)
            mixture = first_v[rows, lanes].astype(jnp.float32) - lambda_ref[h] * second_v[
                rows, lanes
            ].astype(jnp.float32)
            inverse = lax.rsqrt(jnp.mean(mixture * mixture, axis=-1, keepdims=True) + 1e-06)
            normed = (mixture * inverse * gain).astype(jnp.bfloat16)
            term = jnp.dot(normed, basis_v[lanes, :], preferred_element_type=jnp.float32)
            reduced = term if reduced is None else reduced + term
        half_mine_v[t] = reduced[:, :half]
        half_send_v[t] = reduced[:, half:]
        copy = remote(
            half_send_v.at[t],
            half_recv_v.at[t],
            half_send.at[t],
            half_recv.at[t],
            {"tp": other},
        )
        copy.start()
        half_copies.append(copy)
        sends.append(copy)
        if t > 0:
            join_pair(t - 1)
    cot_load.wait()
    arrive(0, 0)
    join_pair(tiles - 1)

    order = (2, 1, 3, 0)
    plane_copies = {}
    for ahead in order:
        at = lax.rem(fs + ahead, line)
        product = jnp.dot(
            turned_v[...],
            cot_v[:, pl.ds(pl.multiple_of(at * shard, shard), shard)],
            preferred_element_type=jnp.float32,
        )
        for part in range(plane):
            piece = product[:, part * quarter : (part + 1) * quarter]
            mine_v[ahead, part] = piece
            plane_send_v[ahead, part] = piece.astype(jnp.bfloat16)
        for step in range(plane - 1):
            copy = remote(
                plane_send_v.at[ahead, peers[step]],
                plane_recv_v.at[step, ahead],
                plane_send.at[step, ahead],
                plane_recv.at[step, ahead],
                {"rep": peers[step]},
            )
            copy.start()
            plane_copies[step, ahead] = copy
            sends.append(copy)

    for c in quarters[1:]:
        arrive(0, c)
    weight_loads[1].wait()
    for c in extras:
        narrow(c)
    for load in moment_loads:
        load.wait()
    my_quarter = pl.ds(pl.multiple_of(rep * quarter, quarter), quarter)
    moment1 = moment1_v[my_quarter].T
    moment2 = moment2_v[my_quarter].T

    line_copies = []
    for ahead in order:
        total = mine_v[ahead, rep]
        for step in range(plane - 1):
            plane_copies[step, ahead].wait_recv()
            total = total + plane_recv_v[step, ahead].astype(jnp.float32)
        if ahead:
            line_send_v[ahead] = total.astype(jnp.bfloat16)
            copy = remote(
                line_send_v.at[ahead],
                line_recv_v.at[ahead],
                line_send.at[ahead],
                line_recv.at[ahead],
                {"fs": lax.rem(fs + ahead, line)},
            )
            copy.start()
            line_copies.append(copy)
            sends.append(copy)

    for c in extras:
        send_own(c)
    for c in quarters[:2]:
        arrive(1, c)

    projected = total
    for copy, ahead in zip(line_copies, order):
        copy.wait_recv()
        projected = projected + line_recv_v[ahead].astype(jnp.float32)
    first_new = beta_first * moment1 + (1.0 - beta_first) * projected
    second_new = beta_second * moment2 + (1.0 - beta_second) * projected * projected
    direction = first_new / (jnp.sqrt(second_new) + 1e-08)
    direction_v[tp, fs, rep] = direction.astype(jnp.bfloat16)
    projected_v[rep] = projected.astype(jnp.bfloat16)

    def spread_line(source, to, at):
        here = direction_v.at[tp, source, rep]
        return remote(here, here, dz_send.at[at], dz_recv.at[source], {"fs": to})

    plane_directions = {}

    def spread_plane(at, source):
        for step in range(plane - 1):
            here = direction_v.at[tp, source, rep]
            copy = remote(
                here, here, dp_send.at[at, step], dp_recv.at[at, step], {"rep": peers[step]}
            )
            copy.start()
            sends.append(copy)

    def to_pair(at, source):
        for step in range(plane - 1):
            here = direction_v.at[tp, source, peers[step]]
            remote(
                here, here, dp_send.at[at, step], dp_recv.at[at, step], {"rep": peers[step]}
            ).wait_recv()
        here = direction_v.at[tp, source]
        copy = remote(here, here, dt_send.at[at], dt_recv.at[at], {"tp": other})
        copy.start()
        sends.append(copy)

    for at, to in enumerate(sources):
        copy = spread_line(fs, to, at)
        copy.start()
        sends.append(copy)
    spread_plane(3, fs)
    proj_copies = []
    for step in range(plane - 1):
        here = projected_v.at[rep]
        copy = remote(
            here, here, proj_send.at[step], proj_recv.at[step], {"rep": peers[step]}
        )
        copy.start()
        sends.append(copy)
        proj_copies.append(copy)

    for c in quarters[2:]:
        arrive(1, c)
    for at, source in enumerate(sources):
        spread_line(source, source, at).wait_recv()
        spread_plane(at, source)
    relay(0)
    for c in quarters:
        arrive(2, c)
    for c in extras:
        arrive(0, c)
    to_pair(3, fs)
    for at, source in enumerate(sources):
        to_pair(at, source)
    relay(1)
    for c in extras:
        arrive(1, c)
    for c in extras:
        arrive(2, c)
    relay(2)

    for load in weight_loads[2:]:
        load.wait()
    for at, source in enumerate(sources + (fs,)):
        here = direction_v.at[other, source]
        remote(here, here, dt_send.at[at], dt_recv.at[at], {"tp": other}).wait_recv()
    energy = jnp.zeros((half, quarter), jnp.float32)
    for at in range(line):
        for part in range(plane):
            lanes = pl.ds((at * plane + part) * quarter, quarter)
            for side in range(2):
                wide = direction_v[side, at, part].astype(jnp.float32)
                energy += wide * wide
            joined_v[:half, lanes] = direction_v[tp, at, part]
            joined_v[half:, lanes] = direction_v[other, at, part]
    total = jnp.sum(jnp.sum(energy, axis=0, keepdims=True), axis=1, keepdims=True)
    spread = jnp.sqrt(total / (width * 2 * half))
    scale = -1.0 / (spread + 1e-06)

    block = values // 4

    def step_block(at, rows):
        return (
            jnp.dot(
                basis_v[rows, :],
                joined_v[:, pl.ds(pl.multiple_of(at * shard, shard), shard)],
                preferred_element_type=jnp.float32,
            )
            * scale
        )

    def columns_of(at):
        return pl.ds(pl.multiple_of(at * shard, shard), shard)

    for b in range(4):
        rows = pl.ds(b * block, block)
        step = step_block(fs, rows)
        fresh = weight_v[rows, :] + step
        step_ref[rows, :] = step
        new_ref[rows, :] = fresh
        copy_ref[rows, columns_of(fs)] = fresh.astype(jnp.bfloat16)
    for copy in proj_copies:
        copy.wait_recv()
    for part in range(plane):
        rows = pl.ds(part * quarter, quarter)
        piece = projected_v[part].astype(jnp.float32).T
        first_new_ref[rows, :] = beta_first * moment1_v[rows, :] + (1.0 - beta_first) * piece
        second_new_ref[rows, :] = (
            beta_second * moment2_v[rows, :] + (1.0 - beta_second) * piece * piece
        )
    for t, source in enumerate(sources):
        finish(t)
        for b in range(4):
            rows = pl.ds(b * block, block)
            copy_ref[rows, columns_of(source)] = (
                gathered_v[source, rows].astype(jnp.float32) + step_block(source, rows)
            ).astype(jnp.bfloat16)
    for copy in sends:
        copy.wait_send()
    for wanted, copy in guarded:

        @pl.when(wanted)
        def _():
            copy.wait_send()


def store_kernel(*refs):
    count = (len(refs) - 1) // 2
    sources, targets, store_sem = refs[:count], refs[count : 2 * count], refs[-1]
    copies = []
    for at in range(count):
        parts = store_sem.shape[1]
        rows = sources[at].shape[0] // parts
        for part in range(parts):
            here = pl.ds(part * rows, rows)
            copies.append(
                pltpu.make_async_copy(
                    sources[at].at[here], targets[at].at[here], store_sem.at[at, part]
                )
            )
    for copy in copies:
        copy.start()
    for copy in copies:
        copy.wait()


def fast_body(
    sizes,
    first_mix,
    second_mix,
    lambda_head,
    head_gain,
    out_cotangent,
    basis,
    weight,
    first_moment,
    second_moment,
):
    line, plane = sizes
    tokens, width = out_cotangent.shape
    values, rank = basis.shape
    shard, half = first_moment.shape
    quarter = shard // plane
    tile = 256 if tokens % 256 == 0 else tokens
    tiles = tokens // tile
    pieces = quarter_chunks + 2
    any_space = pl.BlockSpec(memory_space=pl.ANY)
    on_chip = pl.BlockSpec(memory_space=pltpu.VMEM)
    dma = pltpu.SemaphoreType.DMA
    f32, bf16 = jnp.float32, jnp.bfloat16
    shapes = (
        ((values, width), bf16),
        (weight.shape, f32),
        (weight.shape, f32),
        (first_moment.shape, f32),
        (first_moment.shape, f32),
    )
    held = sum(jnp.dtype(kind).itemsize * shape[0] * shape[1] for shape, kind in shapes)
    fresh = pl.pallas_call(
        functools.partial(exchange_kernel, sizes),
        out_shape=tuple(pltpu.VMEM(shape, kind) for shape, kind in shapes),
        in_specs=[pl.BlockSpec(memory_space=pltpu.SMEM), on_chip] + [any_space] * 7,
        out_specs=(on_chip,) * 5,
        scratch_shapes=[
            pltpu.VMEM(first_mix.shape, bf16),
            pltpu.VMEM(second_mix.shape, bf16),
            pltpu.VMEM(out_cotangent.shape, bf16),
            pltpu.VMEM(basis.shape, bf16),
            pltpu.VMEM(weight.shape, f32),
            pltpu.VMEM((line, values, shard), bf16),
            pltpu.VMEM(first_moment.shape, f32),
            pltpu.VMEM(first_moment.shape, f32),
            pltpu.VMEM((tiles, tile, half), f32),
            pltpu.VMEM((tiles, tile, half), f32),
            pltpu.VMEM((tiles, tile, half), f32),
            pltpu.VMEM((half, tokens), bf16),
            pltpu.VMEM((line, plane, half, quarter), f32),
            pltpu.VMEM((line, plane, half, quarter), bf16),
            pltpu.VMEM((plane - 1, line, half, quarter), bf16),
            pltpu.VMEM((line, half, quarter), bf16),
            pltpu.VMEM((line, half, quarter), bf16),
            pltpu.VMEM((plane, half, quarter), bf16),
            pltpu.VMEM((2, line, plane, half, quarter), bf16),
            pltpu.VMEM((rank, width), bf16),
            dma((9,)),
            dma((tiles, 2)),
            dma((2, pieces)),
            dma((line - 1, pieces)),
            dma((line, pieces)),
            dma((line - 1, quarter_chunks, 2)),
            dma((line - 1, quarter_chunks, 2)),
            dma((line - 1, 2)),
            dma((line - 1, 2)),
            dma((tiles,)),
            dma((tiles,)),
            dma((plane - 1, line)),
            dma((plane - 1, line)),
            dma((line,)),
            dma((line,)),
            dma((plane - 1,)),
            dma((plane - 1,)),
            dma((line - 1,)),
            dma((line,)),
            dma((line, plane - 1)),
            dma((line, plane - 1)),
            dma((line,)),
            dma((line,)),
        ],
        compiler_params=pltpu.CompilerParams(
            collective_id=0, has_side_effects=True, vmem_limit_bytes=vmem_grant - held
        ),
    )(
        lambda_head,
        head_gain.reshape(1, -1),
        first_mix,
        second_mix,
        out_cotangent,
        basis,
        weight,
        first_moment,
        second_moment,
    )
    copied, new, step, first_new, second_new = pl.pallas_call(
        store_kernel,
        out_shape=tuple(jax.ShapeDtypeStruct(shape, kind) for shape, kind in shapes),
        in_specs=[on_chip] * 5,
        out_specs=(any_space,) * 5,
        scratch_shapes=[dma((5, 4))],
        compiler_params=pltpu.CompilerParams(vmem_limit_bytes=vmem_grant // 4),
    )(*(pltpu.with_memory_space_constraint(piece, pltpu.VMEM) for piece in fresh))
    return (new, copied, step, first_new, second_new)


def solution(mesh):
    line, plane, pair = (mesh.shape[name] for name in ("fs", "rep", "tp"))

    def chosen(*args):
        basis, first_moment = args[5], args[7]
        quarter_fits = first_moment.shape[0] % (plane * 128) == 0
        rows_fit = basis.shape[0] % (plane * 16) == 0 and basis.shape[0] % 64 == 0
        rank_fits = pair == 2 and first_moment.shape[1] % 128 == 0
        if line == 4 and plane == 4 and quarter_fits and rows_fit and rank_fits:
            return fast_body((line, plane), *args)
        return body(*args)

    return jax.shard_map(
        chosen,
        mesh=mesh,
        in_specs=(
            P(("fs", "rep"), "tp"),
            P(("fs", "rep"), "tp"),
            P("tp"),
            P(),
            P(("fs", "rep"), None),
            P("tp", None),
            P("tp", "fs"),
            P("fs", "tp"),
            P("fs", "tp"),
        ),
        out_specs=(P("tp", "fs"), P("tp", None), P("tp", "fs"), P("fs", "tp"), P("fs", "tp")),
        check_vma=False,
    )
```

```python
import functools

import jax
import jax.numpy as jnp
from jax import lax
from jax.experimental import pallas as pl
from jax.experimental.pallas import tpu as pltpu
from jax.sharding import PartitionSpec as P

MESH = pl.DeviceIdType.MESH

vmem_grant = 67043328
out_scale = 0.8
beta_first = 0.9
beta_second = 0.95
quarter_chunks = 4
extra_part = 8
own, across = -1, -2
plan = {
    3: ((0, 1), (0, 2), (0, 3),),
    7: ((own, 4), (own, 5), (1, 0), (1, 1),),
    8: ((1, 2), (1, 3),),
    11: ((across, 0), (2, 0), (2, 1), (2, 2), (2, 3), (0, 4), (0, 5),),
    15: ((across, 1), (1, 4), (1, 5), (2, 4), (2, 5), (across, 2),),
    16: ((0, 0),),
}


def head_output(first_piece, second_piece, lambdas, head_gain):
    token_count = first_piece.shape[0]
    head_width = head_gain.shape[0]
    head_count = lambdas.shape[0] // head_width
    mixture = first_piece.astype(jnp.float32) - lambdas[None, :] * second_piece.astype(jnp.float32)
    grouped = mixture.reshape(token_count, head_count, head_width)
    inverse = lax.rsqrt(jnp.mean(grouped * grouped, axis=-1, keepdims=True) + 1e-06)
    normed = grouped * inverse * head_gain[None, None, :] * out_scale
    return normed.reshape(token_count, head_count * head_width).astype(jnp.bfloat16)


def split_product(narrow, wide, numbers):
    upper = wide.astype(jnp.bfloat16)
    lower = (wide - upper.astype(jnp.float32)).astype(jnp.bfloat16)
    return lax.dot_general(
        narrow, upper, numbers, preferred_element_type=jnp.float32
    ) + lax.dot_general(narrow, lower, numbers, preferred_element_type=jnp.float32)


def body(
    first_mix,
    second_mix,
    lambda_head,
    head_gain,
    out_cotangent,
    basis,
    weight,
    first_moment,
    second_moment,
):
    lambdas = jnp.repeat(lambda_head, head_gain.shape[0])
    head_out = head_output(first_mix, second_mix, lambdas, head_gain)
    reduced = jnp.dot(head_out, basis, preferred_element_type=jnp.float32)
    proj_rows = lax.psum_scatter(
        split_product(out_cotangent, reduced, (((0,), (0,)), ((), ()))),
        "fs",
        scatter_dimension=0,
        tiled=True,
    )
    proj_rows = lax.psum_scatter(proj_rows, "tp", scatter_dimension=1, tiled=True)
    projected = lax.psum(proj_rows, "rep")
    first_new = beta_first * first_moment + (1.0 - beta_first) * projected
    second_new = beta_second * second_moment + (1.0 - beta_second) * projected * projected
    direction = first_new / (jnp.sqrt(second_new) + 1e-08)
    energy = lax.psum(jnp.sum(direction * direction), ("fs", "tp"))
    entries = direction.shape[0] * direction.shape[1] * lax.axis_size("fs") * lax.axis_size("tp")
    spread = jnp.sqrt(energy / entries)
    full_direction = lax.all_gather(direction, "tp", axis=1, tiled=True)
    step_out = split_product(basis, full_direction, (((1,), (1,)), ((), ()))) * (
        -1.0 / (spread + 1e-06)
    )
    weight_new = weight + step_out
    weight_copy = lax.all_gather(weight_new.astype(jnp.bfloat16), "fs", axis=1, tiled=True)
    return (weight_new, weight_copy, step_out, first_new, second_new)


def exchange_kernel(
    sizes,
    lambda_hbm,
    gain_hbm,
    first_hbm,
    second_hbm,
    cot_hbm,
    basis_hbm,
    weight_hbm,
    moment1_hbm,
    moment2_hbm,
    copy_ref,
    new_ref,
    step_ref,
    first_new_ref,
    second_new_ref,
    lambda_ref,
    gain_ref,
    first_v,
    second_v,
    cot_v,
    basis_v,
    weight_v,
    gathered_v,
    moment1_v,
    moment2_v,
    half_mine_v,
    half_send_v,
    half_recv_v,
    turned_v,
    mine_v,
    plane_send_v,
    plane_recv_v,
    line_send_v,
    line_recv_v,
    projected_v,
    direction_v,
    joined_v,
    load_sem,
    tile_sem,
    ready_sem,
    wz_send,
    wf_send,
    wz_recv,
    wp_send,
    wp_recv,
    wr_send,
    wr_recv,
    half_send,
    half_recv,
    plane_send,
    plane_recv,
    line_send,
    line_recv,
    proj_send,
    proj_recv,
    dz_send,
    dz_recv,
    dp_send,
    dp_recv,
    dt_send,
    dt_recv,
):
    line, plane = sizes
    fs, rep, tp = lax.axis_index("fs"), lax.axis_index("rep"), lax.axis_index("tp")
    other = 1 - tp
    tokens, width = cot_v.shape
    half, quarter = direction_v.shape[-2:]
    values, shard = weight_v.shape
    quarter_rows = values // plane
    chunk = quarter_rows // quarter_chunks
    head_width = gain_ref.shape[1]
    heads = first_v.shape[1] // head_width
    tiles = tile_sem.shape[0]
    tile = tokens // tiles

    fast_side = rep + 1 - 2 * lax.rem(rep, 2)
    slow_side = lax.rem(rep + 2, 4)
    far_side = 3 - rep
    sides = (fast_side, slow_side)
    peers = (far_side, slow_side, fast_side, rep)

    near_source = 1 + lax.rem(fs, 2)
    last_source = jnp.where(fs < 2, 3, 0)
    sources = (near_source, 6 - fs - near_source - last_source, last_source)
    nexts = tuple(jnp.where(source < fs, fs + 1, fs - 1) for source in sources)
    goes_on = tuple((to >= 0) & (to < line) for to in nexts)

    def remote(source, target, send, recv, where):
        return pltpu.make_async_remote_copy(
            src_ref=source,
            dst_ref=target,
            send_sem=send,
            recv_sem=recv,
            device_id=where,
            device_id_type=MESH,
        )

    def rows_of(owner, start, size):
        return pl.ds(pl.multiple_of(owner * quarter_rows + start, 16), size)

    def weight_load(owner, at):
        rows = rows_of(owner, 0, quarter_rows)
        return pltpu.make_async_copy(weight_hbm.at[rows], weight_v.at[rows], load_sem.at[at])

    weight_loads = [weight_load(owner, at) for at, owner in enumerate((rep, far_side) + sides)]
    basis_loads = [
        pltpu.make_async_copy(
            basis_hbm.at[:, pl.ds(pl.multiple_of(side * half, half), half)],
            basis_v.at[:, pl.ds(at * half, half)],
            load_sem.at[4 + at],
        )
        for at, side in enumerate((tp, other))
    ]
    cot_load = pltpu.make_async_copy(cot_hbm, cot_v, load_sem.at[6])
    moment_loads = [
        pltpu.make_async_copy(moment1_hbm, moment1_v, load_sem.at[7]),
        pltpu.make_async_copy(moment2_hbm, moment2_v, load_sem.at[8]),
    ]
    small_loads = [
        pltpu.make_async_copy(lambda_hbm, lambda_ref, load_sem.at[9]),
        pltpu.make_async_copy(gain_hbm, gain_ref, load_sem.at[10]),
    ]
    weight_loads[0].start()
    for load in small_loads + basis_loads:
        load.start()
    tile_loads = []
    for t in range(tiles):
        rows = pl.ds(t * tile, tile)
        pieces = (
            pltpu.make_async_copy(first_hbm.at[rows], first_v.at[rows], tile_sem.at[t, 0]),
            pltpu.make_async_copy(second_hbm.at[rows], second_v.at[rows], tile_sem.at[t, 1]),
        )
        for piece in pieces:
            piece.start()
        tile_loads.append(pieces)
    cot_load.start()
    weight_loads[1].start()
    for load in moment_loads + weight_loads[2:]:
        load.start()

    near_line = ((fs < line - 1, fs + 1), (fs > 0, fs - 1))
    near_count = jnp.where((fs > 0) & (fs < line - 1), 2, 1)

    def greet_line(semaphore):
        for wanted, to in near_line:

            @pl.when(wanted)
            def _():
                pl.semaphore_signal(
                    semaphore, inc=1, device_id={"fs": to}, device_id_type=MESH
                )

    barrier = pltpu.get_barrier_semaphore()
    greet_line(barrier)
    for step in range(plane - 1):
        pl.semaphore_signal(
            barrier, inc=1, device_id={"rep": peers[step]}, device_id_type=MESH
        )
    pl.semaphore_signal(barrier, inc=1, device_id={"tp": other}, device_id_type=MESH)
    pl.semaphore_wait(barrier, near_count + plane)
    greet_line(ready_sem.at[0])

    sends = []
    guarded = []

    extra = quarter_rows * extra_part // 16
    rest = (quarter_rows - extra) // 2
    pieces = [(rep, c * chunk, chunk) for c in range(quarter_chunks)]
    pieces += [(far_side, c * (extra // 2), extra // 2) for c in range(2)]
    quarters = tuple(range(quarter_chunks))
    extras = (quarter_chunks, quarter_chunks + 1)

    def line_copy(source, c, send, to):
        here = gathered_v.at[source, rows_of(*pieces[c])]
        return remote(here, here, send, wz_recv.at[source, c], {"fs": to})

    def start_if(wanted, copy):
        @pl.when(wanted)
        def _():
            copy.start()

        guarded.append((wanted, copy))

    def narrow(c):
        rows = rows_of(*pieces[c])
        gathered_v[fs, rows] = weight_v[rows].astype(jnp.bfloat16)

    def send_own(c):
        start_if(fs < line - 1, line_copy(fs, c, wz_send.at[0, c], fs + 1))
        start_if(fs > 0, line_copy(fs, c, wz_send.at[1, c], fs - 1))

    def arrive(t, c):
        copy = line_copy(sources[t], c, wf_send.at[t, c], nexts[t])
        copy.wait_recv()
        start_if(goes_on[t], copy)
        if c in quarters:
            here = gathered_v.at[sources[t], rows_of(*pieces[c])]
            for side in range(2):
                copy = remote(
                    here,
                    here,
                    wp_send.at[t, c, side],
                    wp_recv.at[t, c, side],
                    {"rep": sides[side]},
                )
                copy.start()
                sends.append(copy)

    waited = set()

    def from_side(t, c, side):
        if (t, c, side) not in waited:
            waited.add((t, c, side))
            here = gathered_v.at[sources[t], rows_of(sides[side], c * chunk, chunk)]
            remote(
                here,
                here,
                wp_send.at[t, c, side],
                wp_recv.at[t, c, side],
                {"rep": sides[side]},
            ).wait_recv()

    def relay_copy(t, side, owner):
        here = gathered_v.at[sources[t], rows_of(owner, extra + side * rest, rest)]
        return remote(
            here, here, wr_send.at[t, side], wr_recv.at[t, side], {"rep": sides[1 - side]}
        )

    def relay(t):
        for side in range(2):
            from_side(t, (extra + side * rest) // chunk, side)
            copy = relay_copy(t, side, sides[side])
            copy.start()
            sends.append(copy)

    def finish(t):
        for c in quarters:
            for side in range(2):
                from_side(t, c, side)
        for side in range(2):
            relay_copy(t, side, far_side).wait_recv()

    def weave(slot):
        for step in plan.get(slot, ()):
            if step[0] == own:
                send_own(step[1])
            elif step[0] == across:
                relay(step[1])
            else:
                arrive(*step)

    weight_loads[0].wait()
    for c in quarters:
        narrow(c)
        send_own(c)

    for load in basis_loads:
        load.wait()
    for load in small_loads:
        load.wait()
    gain = gain_ref[...] * out_scale
    half_copies = []

    def join_pair(t):
        half_copies[t].wait_recv()
        both = half_mine_v[t] + half_recv_v[t]
        turned_v[:, t * tile : (t + 1) * tile] = both.T.astype(jnp.bfloat16)

    for t in range(tiles):
        for piece in tile_loads[t]:
            piece.wait()
        rows = pl.ds(t * tile, tile)
        reduced = None
        for h in range(heads):
            lanes = pl.ds(h * head_width, head_width)
            mixture = first_v[rows, lanes].astype(jnp.float32) - lambda_ref[h] * second_v[
                rows, lanes
            ].astype(jnp.float32)
            inverse = lax.rsqrt(jnp.mean(mixture * mixture, axis=-1, keepdims=True) + 1e-06)
            normed = (mixture * inverse * gain).astype(jnp.bfloat16)
            term = jnp.dot(normed, basis_v[lanes, :], preferred_element_type=jnp.float32)
            reduced = term if reduced is None else reduced + term
        half_mine_v[t] = reduced[:, :half]
        half_send_v[t] = reduced[:, half:]
        copy = remote(
            half_send_v.at[t],
            half_recv_v.at[t],
            half_send.at[t],
            half_recv.at[t],
            {"tp": other},
        )
        copy.start()
        half_copies.append(copy)
        sends.append(copy)
        if t > 0:
            join_pair(t - 1)
        if t == tiles - 2:
            weave(0)
    pl.semaphore_wait(ready_sem.at[0], near_count)
    greet_line(ready_sem.at[1])
    cot_load.wait()
    weave(16)
    join_pair(tiles - 1)
    weave(1)

    order = (2, 1, 3, 0)
    plane_copies = {}
    for ahead in order:
        at = lax.rem(fs + ahead, line)
        product = jnp.dot(
            turned_v[...],
            cot_v[:, pl.ds(pl.multiple_of(at * shard, shard), shard)],
            preferred_element_type=jnp.float32,
        )
        for part in range(plane):
            piece = product[:, part * quarter : (part + 1) * quarter]
            mine_v[ahead, part] = piece
            plane_send_v[ahead, part] = piece.astype(jnp.bfloat16)
        for step in range(plane - 1):
            copy = remote(
                plane_send_v.at[ahead, peers[step]],
                plane_recv_v.at[step, ahead],
                plane_send.at[step, ahead],
                plane_recv.at[step, ahead],
                {"rep": peers[step]},
            )
            copy.start()
            plane_copies[step, ahead] = copy
            sends.append(copy)
        if ahead == order[1]:
            weave(2)

    weight_loads[1].wait()
    for c in extras:
        narrow(c)
    weave(3)
    for load in moment_loads:
        load.wait()
    my_quarter = pl.ds(pl.multiple_of(rep * quarter, quarter), quarter)
    moment1 = moment1_v[my_quarter].T
    moment2 = moment2_v[my_quarter].T

    pl.semaphore_wait(ready_sem.at[1], near_count)
    line_copies = []
    for ahead in order:
        total = mine_v[ahead, rep]
        for step in range(plane - 1):
            plane_copies[step, ahead].wait_recv()
            total = total + plane_recv_v[step, ahead].astype(jnp.float32)
        if ahead:
            line_send_v[ahead] = total.astype(jnp.bfloat16)
            copy = remote(
                line_send_v.at[ahead],
                line_recv_v.at[ahead],
                line_send.at[ahead],
                line_recv.at[ahead],
                {"fs": lax.rem(fs + ahead, line)},
            )
            copy.start()
            line_copies.append(copy)
            sends.append(copy)
        weave(4 + order.index(ahead))

    projected = total
    for copy, ahead in zip(line_copies, order):
        copy.wait_recv()
        projected = projected + line_recv_v[ahead].astype(jnp.float32)
    first_new = beta_first * moment1 + (1.0 - beta_first) * projected
    second_new = beta_second * moment2 + (1.0 - beta_second) * projected * projected
    direction = first_new / (jnp.sqrt(second_new) + 1e-08)
    direction_v[tp, fs, rep] = direction.astype(jnp.bfloat16)
    projected_v[rep] = projected.astype(jnp.bfloat16)

    def spread_line(source, to, at):
        here = direction_v.at[tp, source, rep]
        return remote(here, here, dz_send.at[at], dz_recv.at[source], {"fs": to})

    plane_directions = {}

    def spread_plane(at, source):
        for step in range(plane - 1):
            here = direction_v.at[tp, source, rep]
            copy = remote(
                here, here, dp_send.at[at, step], dp_recv.at[at, step], {"rep": peers[step]}
            )
            copy.start()
            sends.append(copy)

    def to_pair(at, source):
        for step in range(plane - 1):
            here = direction_v.at[tp, source, peers[step]]
            remote(
                here, here, dp_send.at[at, step], dp_recv.at[at, step], {"rep": peers[step]}
            ).wait_recv()
        here = direction_v.at[tp, source]
        copy = remote(here, here, dt_send.at[at], dt_recv.at[at], {"tp": other})
        copy.start()
        sends.append(copy)

    for at, to in enumerate(sources):
        copy = spread_line(fs, to, at)
        copy.start()
        sends.append(copy)
    spread_plane(3, fs)
    proj_copies = []
    for step in range(plane - 1):
        here = projected_v.at[rep]
        copy = remote(
            here, here, proj_send.at[step], proj_recv.at[step], {"rep": peers[step]}
        )
        copy.start()
        sends.append(copy)
        proj_copies.append(copy)

    weave(8)
    for at, source in enumerate(sources):
        spread_line(source, source, at).wait_recv()
        spread_plane(at, source)
        weave(9 + at)
    to_pair(3, fs)
    weave(12)
    for at, source in enumerate(sources):
        to_pair(at, source)
        weave(13 + at)

    for load in weight_loads[2:]:
        load.wait()
    for at, source in enumerate(sources + (fs,)):
        here = direction_v.at[other, source]
        remote(here, here, dt_send.at[at], dt_recv.at[at], {"tp": other}).wait_recv()
    energy = jnp.zeros((half, quarter), jnp.float32)
    for at in range(line):
        for part in range(plane):
            lanes = pl.ds((at * plane + part) * quarter, quarter)
            for side in range(2):
                wide = direction_v[side, at, part].astype(jnp.float32)
                energy += wide * wide
            joined_v[:half, lanes] = direction_v[tp, at, part]
            joined_v[half:, lanes] = direction_v[other, at, part]
    total = jnp.sum(jnp.sum(energy, axis=0, keepdims=True), axis=1, keepdims=True)
    spread = jnp.sqrt(total / (width * 2 * half))
    scale = -1.0 / (spread + 1e-06)

    block = values // 4

    def step_block(at, rows):
        return (
            jnp.dot(
                basis_v[rows, :],
                joined_v[:, pl.ds(pl.multiple_of(at * shard, shard), shard)],
                preferred_element_type=jnp.float32,
            )
            * scale
        )

    def columns_of(at):
        return pl.ds(pl.multiple_of(at * shard, shard), shard)

    for b in range(4):
        rows = pl.ds(b * block, block)
        step = step_block(fs, rows)
        fresh = weight_v[rows, :] + step
        step_ref[rows, :] = step
        new_ref[rows, :] = fresh
        copy_ref[rows, columns_of(fs)] = fresh.astype(jnp.bfloat16)
    for copy in proj_copies:
        copy.wait_recv()
    for part in range(plane):
        rows = pl.ds(part * quarter, quarter)
        piece = projected_v[part].astype(jnp.float32).T
        first_new_ref[rows, :] = beta_first * moment1_v[rows, :] + (1.0 - beta_first) * piece
        second_new_ref[rows, :] = (
            beta_second * moment2_v[rows, :] + (1.0 - beta_second) * piece * piece
        )
    for t, source in enumerate(sources):
        finish(t)
        for b in range(4):
            rows = pl.ds(b * block, block)
            copy_ref[rows, columns_of(source)] = (
                gathered_v[source, rows].astype(jnp.float32) + step_block(source, rows)
            ).astype(jnp.bfloat16)
    for copy in sends:
        copy.wait_send()
    for wanted, copy in guarded:

        @pl.when(wanted)
        def _():
            copy.wait_send()


def store_kernel(*refs):
    count = (len(refs) - 1) // 2
    sources, targets, store_sem = refs[:count], refs[count : 2 * count], refs[-1]
    copies = []
    for at in range(count):
        parts = store_sem.shape[1]
        rows = sources[at].shape[0] // parts
        for part in range(parts):
            here = pl.ds(part * rows, rows)
            copies.append(
                pltpu.make_async_copy(
                    sources[at].at[here], targets[at].at[here], store_sem.at[at, part]
                )
            )
    for copy in copies:
        copy.start()
    for copy in copies:
        copy.wait()


def fast_body(
    sizes,
    first_mix,
    second_mix,
    lambda_head,
    head_gain,
    out_cotangent,
    basis,
    weight,
    first_moment,
    second_moment,
):
    line, plane = sizes
    tokens, width = out_cotangent.shape
    values, rank = basis.shape
    shard, half = first_moment.shape
    quarter = shard // plane
    tile = 256 if tokens % 256 == 0 else tokens
    tiles = tokens // tile
    pieces = quarter_chunks + 2
    any_space = pl.BlockSpec(memory_space=pl.ANY)
    on_chip = pl.BlockSpec(memory_space=pltpu.VMEM)
    dma = pltpu.SemaphoreType.DMA
    f32, bf16 = jnp.float32, jnp.bfloat16
    shapes = (
        ((values, width), bf16),
        (weight.shape, f32),
        (weight.shape, f32),
        (first_moment.shape, f32),
        (first_moment.shape, f32),
    )
    held = sum(jnp.dtype(kind).itemsize * shape[0] * shape[1] for shape, kind in shapes)
    fresh = pl.pallas_call(
        functools.partial(exchange_kernel, sizes),
        out_shape=tuple(pltpu.VMEM(shape, kind) for shape, kind in shapes),
        in_specs=[any_space] * 9,
        out_specs=(on_chip,) * 5,
        scratch_shapes=[
            pltpu.SMEM(lambda_head.shape, f32),
            pltpu.VMEM((1, head_gain.shape[0]), f32),
            pltpu.VMEM(first_mix.shape, bf16),
            pltpu.VMEM(second_mix.shape, bf16),
            pltpu.VMEM(out_cotangent.shape, bf16),
            pltpu.VMEM(basis.shape, bf16),
            pltpu.VMEM(weight.shape, f32),
            pltpu.VMEM((line, values, shard), bf16),
            pltpu.VMEM(first_moment.shape, f32),
            pltpu.VMEM(first_moment.shape, f32),
            pltpu.VMEM((tiles, tile, half), f32),
            pltpu.VMEM((tiles, tile, half), f32),
            pltpu.VMEM((tiles, tile, half), f32),
            pltpu.VMEM((half, tokens), bf16),
            pltpu.VMEM((line, plane, half, quarter), f32),
            pltpu.VMEM((line, plane, half, quarter), bf16),
            pltpu.VMEM((plane - 1, line, half, quarter), bf16),
            pltpu.VMEM((line, half, quarter), bf16),
            pltpu.VMEM((line, half, quarter), bf16),
            pltpu.VMEM((plane, half, quarter), bf16),
            pltpu.VMEM((2, line, plane, half, quarter), bf16),
            pltpu.VMEM((rank, width), bf16),
            dma((11,)),
            dma((tiles, 2)),
            pltpu.SemaphoreType.REGULAR((2,)),
            dma((2, pieces)),
            dma((line - 1, pieces)),
            dma((line, pieces)),
            dma((line - 1, quarter_chunks, 2)),
            dma((line - 1, quarter_chunks, 2)),
            dma((line - 1, 2)),
            dma((line - 1, 2)),
            dma((tiles,)),
            dma((tiles,)),
            dma((plane - 1, line)),
            dma((plane - 1, line)),
            dma((line,)),
            dma((line,)),
            dma((plane - 1,)),
            dma((plane - 1,)),
            dma((line - 1,)),
            dma((line,)),
            dma((line, plane - 1)),
            dma((line, plane - 1)),
            dma((line,)),
            dma((line,)),
        ],
        compiler_params=pltpu.CompilerParams(
            collective_id=0, has_side_effects=True, vmem_limit_bytes=vmem_grant - held
        ),
    )(
        lambda_head,
        head_gain.reshape(1, -1),
        first_mix,
        second_mix,
        out_cotangent,
        basis,
        weight,
        first_moment,
        second_moment,
    )
    copied, new, step, first_new, second_new = pl.pallas_call(
        store_kernel,
        out_shape=tuple(jax.ShapeDtypeStruct(shape, kind) for shape, kind in shapes),
        in_specs=[on_chip] * 5,
        out_specs=(any_space,) * 5,
        scratch_shapes=[dma((5, 4))],
        compiler_params=pltpu.CompilerParams(vmem_limit_bytes=vmem_grant // 4),
    )(*(pltpu.with_memory_space_constraint(piece, pltpu.VMEM) for piece in fresh))
    return (new, copied, step, first_new, second_new)


def solution(mesh):
    line, plane, pair = (mesh.shape[name] for name in ("fs", "rep", "tp"))

    def chosen(*args):
        basis, first_moment = args[5], args[7]
        quarter_fits = first_moment.shape[0] % (plane * 128) == 0
        rows_fit = basis.shape[0] % (plane * 16) == 0 and basis.shape[0] % 64 == 0
        rank_fits = pair == 2 and first_moment.shape[1] % 128 == 0
        if line == 4 and plane == 4 and quarter_fits and rows_fit and rank_fits:
            return fast_body((line, plane), *args)
        return body(*args)

    return jax.shard_map(
        chosen,
        mesh=mesh,
        in_specs=(
            P(("fs", "rep"), "tp"),
            P(("fs", "rep"), "tp"),
            P("tp"),
            P(),
            P(("fs", "rep"), None),
            P("tp", None),
            P("tp", "fs"),
            P("fs", "tp"),
            P("fs", "tp"),
        ),
        out_specs=(P("tp", "fs"), P("tp", None), P("tp", "fs"), P("fs", "tp"), P("fs", "tp")),
        check_vma=False,
    )
```

```python
import functools

import jax
import jax.numpy as jnp
from jax import lax
from jax.experimental import pallas as pl
from jax.experimental.pallas import tpu as pltpu
from jax.sharding import PartitionSpec as P

MESH = pl.DeviceIdType.MESH

vmem_grant = 67043328
out_scale = 0.8
beta_first = 0.9
beta_second = 0.95
quarter_chunks = 4
extra_part = 10
own, across, turned, kept = -1, -2, -3, -4
plan = {
    16: ((own, 5),),
    17: ((own, 4), (0, 0),),
    4: ((0, 2),),
    6: ((0, 3),),
    7: ((0, 1), (1, 2),),
    8: ((kept,), (turned, 3), (1, 3), (0, 4),),
    11: (
        (1, 0),
        (2, 2),
        (turned, 1),
        (2, 3),
        (turned, 2),
        (1, 4),
        (turned, 0),
        (across, 1),
        (0, 5),
    ),
    12: ((1, 1), (2, 0), (across, 0), (1, 5), (2, 4), (2, 1), (across, 2),),
    15: ((2, 5),),
}


def head_output(first_piece, second_piece, lambdas, head_gain):
    token_count = first_piece.shape[0]
    head_width = head_gain.shape[0]
    head_count = lambdas.shape[0] // head_width
    mixture = first_piece.astype(jnp.float32) - lambdas[None, :] * second_piece.astype(jnp.float32)
    grouped = mixture.reshape(token_count, head_count, head_width)
    inverse = lax.rsqrt(jnp.mean(grouped * grouped, axis=-1, keepdims=True) + 1e-06)
    normed = grouped * inverse * head_gain[None, None, :] * out_scale
    return normed.reshape(token_count, head_count * head_width).astype(jnp.bfloat16)


def split_product(narrow, wide, numbers):
    upper = wide.astype(jnp.bfloat16)
    lower = (wide - upper.astype(jnp.float32)).astype(jnp.bfloat16)
    return lax.dot_general(
        narrow, upper, numbers, preferred_element_type=jnp.float32
    ) + lax.dot_general(narrow, lower, numbers, preferred_element_type=jnp.float32)


def body(
    first_mix,
    second_mix,
    lambda_head,
    head_gain,
    out_cotangent,
    basis,
    weight,
    first_moment,
    second_moment,
):
    lambdas = jnp.repeat(lambda_head, head_gain.shape[0])
    head_out = head_output(first_mix, second_mix, lambdas, head_gain)
    reduced = jnp.dot(head_out, basis, preferred_element_type=jnp.float32)
    proj_rows = lax.psum_scatter(
        split_product(out_cotangent, reduced, (((0,), (0,)), ((), ()))),
        "fs",
        scatter_dimension=0,
        tiled=True,
    )
    proj_rows = lax.psum_scatter(proj_rows, "tp", scatter_dimension=1, tiled=True)
    projected = lax.psum(proj_rows, "rep")
    first_new = beta_first * first_moment + (1.0 - beta_first) * projected
    second_new = beta_second * second_moment + (1.0 - beta_second) * projected * projected
    direction = first_new / (jnp.sqrt(second_new) + 1e-08)
    energy = lax.psum(jnp.sum(direction * direction), ("fs", "tp"))
    entries = direction.shape[0] * direction.shape[1] * lax.axis_size("fs") * lax.axis_size("tp")
    spread = jnp.sqrt(energy / entries)
    full_direction = lax.all_gather(direction, "tp", axis=1, tiled=True)
    step_out = split_product(basis, full_direction, (((1,), (1,)), ((), ()))) * (
        -1.0 / (spread + 1e-06)
    )
    weight_new = weight + step_out
    weight_copy = lax.all_gather(weight_new.astype(jnp.bfloat16), "fs", axis=1, tiled=True)
    return (weight_new, weight_copy, step_out, first_new, second_new)


def exchange_kernel(
    sizes,
    lambda_hbm,
    gain_hbm,
    first_hbm,
    second_hbm,
    cot_hbm,
    basis_hbm,
    weight_hbm,
    moment1_hbm,
    moment2_hbm,
    copy_ref,
    new_ref,
    step_ref,
    first_new_ref,
    second_new_ref,
    lambda_ref,
    gain_ref,
    first_v,
    second_v,
    cot_v,
    basis_v,
    weight_v,
    gathered_v,
    moment1_v,
    moment2_v,
    half_mine_v,
    half_send_v,
    half_recv_v,
    turned_v,
    mine_v,
    across_send_v,
    across_recv_v,
    joint_send_v,
    joint_recv_v,
    line_send_v,
    line_recv_v,
    projected_v,
    direction_v,
    joined_v,
    load_sem,
    tile_sem,
    ready_sem,
    wz_send,
    wf_send,
    wz_recv,
    wp_send,
    wp_recv,
    wr_send,
    wr_recv,
    half_send,
    half_recv,
    across_send,
    across_recv,
    joint_send,
    joint_recv,
    line_send,
    line_recv,
    proj_send,
    proj_recv,
    dz_send,
    dz_recv,
    dp_send,
    dp_recv,
    dr_send,
    dr_recv,
    dt_send,
    dt_recv,
):
    line, plane = sizes
    fs, rep, tp = lax.axis_index("fs"), lax.axis_index("rep"), lax.axis_index("tp")
    other = 1 - tp
    tokens, width = cot_v.shape
    half, quarter = direction_v.shape[-2:]
    values, shard = weight_v.shape
    quarter_rows = values // plane
    chunk = quarter_rows // quarter_chunks
    head_width = gain_ref.shape[1]
    heads = first_v.shape[1] // head_width
    tiles = tile_sem.shape[0]
    tile = tokens // tiles

    fast_side = rep + 1 - 2 * lax.rem(rep, 2)
    slow_side = lax.rem(rep + 2, 4)
    far_side = 3 - rep
    sides = (fast_side, slow_side)
    peers = (far_side, slow_side, fast_side, rep)

    near_source = 1 + lax.rem(fs, 2)
    last_source = jnp.where(fs < 2, 3, 0)
    sources = (near_source, 6 - fs - near_source - last_source, last_source)
    nexts = tuple(jnp.where(source < fs, fs + 1, fs - 1) for source in sources)
    goes_on = tuple((to >= 0) & (to < line) for to in nexts)

    def remote(source, target, send, recv, where):
        return pltpu.make_async_remote_copy(
            src_ref=source,
            dst_ref=target,
            send_sem=send,
            recv_sem=recv,
            device_id=where,
            device_id_type=MESH,
        )

    def rows_of(owner, start, size):
        return pl.ds(pl.multiple_of(owner * quarter_rows + start, 16), size)

    def weight_load(owner, at):
        rows = rows_of(owner, 0, quarter_rows)
        return pltpu.make_async_copy(weight_hbm.at[rows], weight_v.at[rows], load_sem.at[at])

    weight_loads = [weight_load(owner, at) for at, owner in enumerate((rep, far_side) + sides)]
    basis_loads = [
        pltpu.make_async_copy(
            basis_hbm.at[:, pl.ds(pl.multiple_of(side * half, half), half)],
            basis_v.at[:, pl.ds(at * half, half)],
            load_sem.at[4 + at],
        )
        for at, side in enumerate((tp, other))
    ]
    cot_load = pltpu.make_async_copy(cot_hbm, cot_v, load_sem.at[6])
    moment_loads = [
        pltpu.make_async_copy(moment1_hbm, moment1_v, load_sem.at[7]),
        pltpu.make_async_copy(moment2_hbm, moment2_v, load_sem.at[8]),
    ]
    small_loads = [
        pltpu.make_async_copy(lambda_hbm, lambda_ref, load_sem.at[9]),
        pltpu.make_async_copy(gain_hbm, gain_ref, load_sem.at[10]),
    ]
    weight_loads[0].start()
    for load in small_loads + basis_loads:
        load.start()
    tile_loads = []
    for t in range(tiles):
        rows = pl.ds(t * tile, tile)
        pieces = (
            pltpu.make_async_copy(first_hbm.at[rows], first_v.at[rows], tile_sem.at[t, 0]),
            pltpu.make_async_copy(second_hbm.at[rows], second_v.at[rows], tile_sem.at[t, 1]),
        )
        for piece in pieces:
            piece.start()
        tile_loads.append(pieces)
    cot_load.start()
    weight_loads[1].start()
    for load in moment_loads + weight_loads[2:]:
        load.start()

    near_line = ((fs < line - 1, fs + 1), (fs > 0, fs - 1))
    near_count = jnp.where((fs > 0) & (fs < line - 1), 2, 1)

    def greet_line(semaphore):
        for wanted, to in near_line:

            @pl.when(wanted)
            def _():
                pl.semaphore_signal(
                    semaphore, inc=1, device_id={"fs": to}, device_id_type=MESH
                )

    barrier = pltpu.get_barrier_semaphore()
    greet_line(barrier)
    for step in range(plane - 1):
        pl.semaphore_signal(
            barrier, inc=1, device_id={"rep": peers[step]}, device_id_type=MESH
        )
    pl.semaphore_signal(barrier, inc=1, device_id={"tp": other}, device_id_type=MESH)
    pl.semaphore_wait(barrier, near_count + plane)
    greet_line(ready_sem.at[0])

    sends = []
    guarded = []

    extra = quarter_rows * extra_part // 16
    rest = (quarter_rows - extra) // 2
    pieces = [(rep, c * chunk, chunk) for c in range(quarter_chunks)]
    pieces += [(far_side, c * (extra // 2), extra // 2) for c in range(2)]
    quarters = tuple(range(quarter_chunks))
    extras = (quarter_chunks, quarter_chunks + 1)

    def line_copy(source, c, send, to):
        here = gathered_v.at[source, rows_of(*pieces[c])]
        return remote(here, here, send, wz_recv.at[source, c], {"fs": to})

    def start_if(wanted, copy):
        @pl.when(wanted)
        def _():
            copy.start()

        guarded.append((wanted, copy))

    def narrow(c):
        rows = rows_of(*pieces[c])
        gathered_v[fs, rows] = weight_v[rows].astype(jnp.bfloat16)

    def send_own(c):
        start_if(fs < line - 1, line_copy(fs, c, wz_send.at[0, c], fs + 1))
        start_if(fs > 0, line_copy(fs, c, wz_send.at[1, c], fs - 1))

    def arrive(t, c):
        copy = line_copy(sources[t], c, wf_send.at[t, c], nexts[t])
        copy.wait_recv()
        start_if(goes_on[t], copy)
        if c in quarters:
            here = gathered_v.at[sources[t], rows_of(*pieces[c])]
            for side in range(2):
                copy = remote(
                    here,
                    here,
                    wp_send.at[t, c, side],
                    wp_recv.at[t, c, side],
                    {"rep": sides[side]},
                )
                copy.start()
                sends.append(copy)

    waited = set()

    def from_side(t, c, side):
        if (t, c, side) not in waited:
            waited.add((t, c, side))
            here = gathered_v.at[sources[t], rows_of(sides[side], c * chunk, chunk)]
            remote(
                here,
                here,
                wp_send.at[t, c, side],
                wp_recv.at[t, c, side],
                {"rep": sides[side]},
            ).wait_recv()

    def relay_copy(t, side, owner):
        here = gathered_v.at[sources[t], rows_of(owner, extra + side * rest, rest)]
        return remote(
            here, here, wr_send.at[t, side], wr_recv.at[t, side], {"rep": sides[1 - side]}
        )

    def relay(t):
        for side in range(2):
            start = extra + side * rest
            for c in range(start // chunk, -(-(start + rest) // chunk)):
                from_side(t, c, side)
            copy = relay_copy(t, side, sides[side])
            copy.start()
            sends.append(copy)

    def finish(t):
        for c in quarters:
            for side in range(2):
                from_side(t, c, side)
        for side in range(2):
            relay_copy(t, side, far_side).wait_recv()

    def weave(slot):
        for step in plan.get(slot, ()):
            if step[0] == own:
                send_own(step[1])
            elif step[0] == across:
                relay(step[1])
            elif step[0] == turned:
                relay_direction(step[1])
            elif step[0] == kept:
                spread_projected()
            else:
                arrive(*step)

    weight_loads[0].wait()
    for c in quarters:
        narrow(c)
        send_own(c)

    for load in basis_loads:
        load.wait()
    for load in small_loads:
        load.wait()
    gain = gain_ref[...] * out_scale
    half_copies = []

    def join_pair(t):
        half_copies[t].wait_recv()
        both = half_mine_v[t] + half_recv_v[t]
        turned_v[:, t * tile : (t + 1) * tile] = both.T.astype(jnp.bfloat16)

    for t in range(tiles):
        for piece in tile_loads[t]:
            piece.wait()
        rows = pl.ds(t * tile, tile)
        reduced = None
        for h in range(heads):
            lanes = pl.ds(h * head_width, head_width)
            mixture = first_v[rows, lanes].astype(jnp.float32) - lambda_ref[h] * second_v[
                rows, lanes
            ].astype(jnp.float32)
            inverse = lax.rsqrt(jnp.mean(mixture * mixture, axis=-1, keepdims=True) + 1e-06)
            normed = (mixture * inverse * gain).astype(jnp.bfloat16)
            term = jnp.dot(normed, basis_v[lanes, :], preferred_element_type=jnp.float32)
            reduced = term if reduced is None else reduced + term
        half_mine_v[t] = reduced[:, :half]
        half_send_v[t] = reduced[:, half:]
        copy = remote(
            half_send_v.at[t],
            half_recv_v.at[t],
            half_send.at[t],
            half_recv.at[t],
            {"tp": other},
        )
        copy.start()
        half_copies.append(copy)
        sends.append(copy)
        if t > 0:
            join_pair(t - 1)
        if t == tiles - 2:
            weave(0)
    pl.semaphore_wait(ready_sem.at[0], near_count)
    greet_line(ready_sem.at[1])
    weight_loads[1].wait()
    for c in extras:
        narrow(c)
    cot_load.wait()
    weave(16)
    join_pair(tiles - 1)
    weave(1)

    order = (2, 1, 3, 0)
    middle = half // 2
    halves = (pl.ds(0, middle), pl.ds(middle, middle))
    bits = (lax.rem(rep, 2), lax.div(rep, 2))
    across_copies = {}
    joint_copies = {}
    for ahead in order:
        at = lax.rem(fs + ahead, line)
        product = jnp.dot(
            turned_v[...],
            cot_v[:, pl.ds(pl.multiple_of(at * shard, shard), shard)],
            preferred_element_type=jnp.float32,
        )
        for part in range(plane):
            piece = product[:, part * quarter : (part + 1) * quarter]
            mine_v[ahead, part] = piece
            piece = piece.astype(jnp.bfloat16)
            across_send_v[0, ahead, part % 2, part // 2] = piece[:middle]
            across_send_v[1, ahead, part // 2, part % 2] = piece[middle:]
        for side in range(2):
            copy = remote(
                across_send_v.at[side, ahead, 1 - bits[side]],
                across_recv_v.at[side, ahead],
                across_send.at[side, ahead],
                across_recv.at[side, ahead],
                {"rep": sides[side]},
            )
            copy.start()
            across_copies[side, ahead] = copy
            sends.append(copy)
        if ahead == order[1]:
            weave(2)

    weave(3)
    for load in moment_loads:
        load.wait()
    my_quarter = pl.ds(pl.multiple_of(rep * quarter, quarter), quarter)
    moment1 = moment1_v[my_quarter].T
    moment2 = moment2_v[my_quarter].T

    for ahead in order:
        for side in range(2):
            across_copies[side, ahead].wait_recv()
            turn = 1 - side
            joint = (
                mine_v[ahead, sides[turn], halves[side]]
                + across_recv_v[side, ahead, 1 - bits[turn]].astype(jnp.float32)
            )
            joint_send_v[side, ahead] = joint.astype(jnp.bfloat16)
            copy = remote(
                joint_send_v.at[side, ahead],
                joint_recv_v.at[side, ahead],
                joint_send.at[side, ahead],
                joint_recv.at[side, ahead],
                {"rep": sides[turn]},
            )
            copy.start()
            joint_copies[side, ahead] = copy
            sends.append(copy)
        weave(17 + order.index(ahead))
    pl.semaphore_wait(ready_sem.at[1], near_count)
    line_copies = []
    for ahead in order:
        totals = []
        for side in range(2):
            joint_copies[side, ahead].wait_recv()
            totals.append(
                mine_v[ahead, rep, halves[side]]
                + across_recv_v[side, ahead, bits[1 - side]].astype(jnp.float32)
                + joint_recv_v[side, ahead].astype(jnp.float32)
            )
        total = jnp.concatenate(totals, axis=0)
        if ahead:
            line_send_v[ahead] = total.astype(jnp.bfloat16)
            copy = remote(
                line_send_v.at[ahead],
                line_recv_v.at[ahead],
                line_send.at[ahead],
                line_recv.at[ahead],
                {"fs": lax.rem(fs + ahead, line)},
            )
            copy.start()
            line_copies.append(copy)
            sends.append(copy)
        weave(4 + order.index(ahead))

    projected = total
    for copy, ahead in zip(line_copies, order):
        copy.wait_recv()
        projected = projected + line_recv_v[ahead].astype(jnp.float32)
    first_new = beta_first * moment1 + (1.0 - beta_first) * projected
    second_new = beta_second * moment2 + (1.0 - beta_second) * projected * projected
    direction = first_new / (jnp.sqrt(second_new) + 1e-08)
    direction_v[tp, fs, rep] = direction.astype(jnp.bfloat16)
    projected_v[rep] = projected.astype(jnp.bfloat16)

    def spread_line(source, to, at):
        here = direction_v.at[tp, source, rep]
        return remote(here, here, dz_send.at[at], dz_recv.at[source], {"fs": to})

    def spread_plane(at, source):
        for side in range(2):
            here = direction_v.at[tp, source, rep]
            copy = remote(
                here, here, dp_send.at[at, side], dp_recv.at[at, side], {"rep": sides[side]}
            )
            copy.start()
            sends.append(copy)

    def spread_relay_copy(at, side, owner):
        here = direction_v.at[tp, (sources + (fs,))[at], owner, halves[side]]
        return remote(
            here, here, dr_send.at[at, side], dr_recv.at[at, side], {"rep": sides[1 - side]}
        )

    def relay_direction(at):
        for side in range(2):
            here = direction_v.at[tp, (sources + (fs,))[at], sides[side]]
            remote(
                here, here, dp_send.at[at, side], dp_recv.at[at, side], {"rep": sides[side]}
            ).wait_recv()
            copy = spread_relay_copy(at, side, sides[side])
            copy.start()
            sends.append(copy)

    def to_pair(at, source):
        for side in range(2):
            spread_relay_copy(at, side, far_side).wait_recv()
        here = direction_v.at[tp, source]
        copy = remote(here, here, dt_send.at[at], dt_recv.at[at], {"tp": other})
        copy.start()
        sends.append(copy)

    for at, to in enumerate(sources):
        copy = spread_line(fs, to, at)
        copy.start()
        sends.append(copy)
    spread_plane(3, fs)
    proj_copies = []

    def spread_projected():
        for step in range(plane - 1):
            here = projected_v.at[rep]
            copy = remote(
                here, here, proj_send.at[step], proj_recv.at[step], {"rep": peers[step]}
            )
            copy.start()
            sends.append(copy)
            proj_copies.append(copy)

    weave(8)
    for at, source in enumerate(sources):
        spread_line(source, source, at).wait_recv()
        spread_plane(at, source)
        weave(9 + at)
    to_pair(3, fs)
    weave(12)
    for at, source in enumerate(sources):
        to_pair(at, source)
        weave(13 + at)

    for at, source in enumerate(sources + (fs,)):
        here = direction_v.at[other, source]
        remote(here, here, dt_send.at[at], dt_recv.at[at], {"tp": other}).wait_recv()
    energy = jnp.zeros((half, quarter), jnp.float32)
    for at in range(line):
        for part in range(plane):
            lanes = pl.ds((at * plane + part) * quarter, quarter)
            for side in range(2):
                wide = direction_v[side, at, part].astype(jnp.float32)
                energy += wide * wide
            joined_v[:half, lanes] = direction_v[tp, at, part]
            joined_v[half:, lanes] = direction_v[other, at, part]
    total = jnp.sum(jnp.sum(energy, axis=0, keepdims=True), axis=1, keepdims=True)
    spread = jnp.sqrt(total / (width * 2 * half))
    scale = -1.0 / (spread + 1e-06)
    weave(21)

    block = values // 4

    def step_block(at, rows):
        return (
            jnp.dot(
                basis_v[rows, :],
                joined_v[:, pl.ds(pl.multiple_of(at * shard, shard), shard)],
                preferred_element_type=jnp.float32,
            )
            * scale
        )

    def columns_of(at):
        return pl.ds(pl.multiple_of(at * shard, shard), shard)

    for load in weight_loads[2:]:
        load.wait()
    for b in range(4):
        rows = pl.ds(b * block, block)
        step = step_block(fs, rows)
        fresh = weight_v[rows, :] + step
        step_ref[rows, :] = step
        new_ref[rows, :] = fresh
        copy_ref[rows, columns_of(fs)] = fresh.astype(jnp.bfloat16)
    for copy in proj_copies:
        copy.wait_recv()
    for part in range(plane):
        rows = pl.ds(part * quarter, quarter)
        piece = projected_v[part].astype(jnp.float32).T
        first_new_ref[rows, :] = beta_first * moment1_v[rows, :] + (1.0 - beta_first) * piece
        second_new_ref[rows, :] = (
            beta_second * moment2_v[rows, :] + (1.0 - beta_second) * piece * piece
        )
    weave(22)
    for t, source in enumerate(sources):
        finish(t)
        for b in range(4):
            rows = pl.ds(b * block, block)
            copy_ref[rows, columns_of(source)] = (
                gathered_v[source, rows].astype(jnp.float32) + step_block(source, rows)
            ).astype(jnp.bfloat16)
        weave(23 + t)
    for copy in sends:
        copy.wait_send()
    for wanted, copy in guarded:

        @pl.when(wanted)
        def _():
            copy.wait_send()


def store_kernel(*refs):
    count = (len(refs) - 1) // 2
    sources, targets, store_sem = refs[:count], refs[count : 2 * count], refs[-1]
    copies = []
    for at in range(count):
        parts = store_sem.shape[1]
        rows = sources[at].shape[0] // parts
        for part in range(parts):
            here = pl.ds(part * rows, rows)
            copies.append(
                pltpu.make_async_copy(
                    sources[at].at[here], targets[at].at[here], store_sem.at[at, part]
                )
            )
    for copy in copies:
        copy.start()
    for copy in copies:
        copy.wait()


def fast_body(
    sizes,
    first_mix,
    second_mix,
    lambda_head,
    head_gain,
    out_cotangent,
    basis,
    weight,
    first_moment,
    second_moment,
):
    line, plane = sizes
    tokens, width = out_cotangent.shape
    values, rank = basis.shape
    shard, half = first_moment.shape
    quarter = shard // plane
    tile = 256 if tokens % 256 == 0 else tokens
    tiles = tokens // tile
    pieces = quarter_chunks + 2
    any_space = pl.BlockSpec(memory_space=pl.ANY)
    on_chip = pl.BlockSpec(memory_space=pltpu.VMEM)
    dma = pltpu.SemaphoreType.DMA
    f32, bf16 = jnp.float32, jnp.bfloat16
    shapes = (
        ((values, width), bf16),
        (weight.shape, f32),
        (weight.shape, f32),
        (first_moment.shape, f32),
        (first_moment.shape, f32),
    )
    held = sum(jnp.dtype(kind).itemsize * shape[0] * shape[1] for shape, kind in shapes)
    fresh = pl.pallas_call(
        functools.partial(exchange_kernel, sizes),
        out_shape=tuple(pltpu.VMEM(shape, kind) for shape, kind in shapes),
        in_specs=[any_space] * 9,
        out_specs=(on_chip,) * 5,
        scratch_shapes=[
            pltpu.SMEM(lambda_head.shape, f32),
            pltpu.VMEM((1, head_gain.shape[0]), f32),
            pltpu.VMEM(first_mix.shape, bf16),
            pltpu.VMEM(second_mix.shape, bf16),
            pltpu.VMEM(out_cotangent.shape, bf16),
            pltpu.VMEM(basis.shape, bf16),
            pltpu.VMEM(weight.shape, f32),
            pltpu.VMEM((line, values, shard), bf16),
            pltpu.VMEM(first_moment.shape, f32),
            pltpu.VMEM(first_moment.shape, f32),
            pltpu.VMEM((tiles, tile, half), f32),
            pltpu.VMEM((tiles, tile, half), f32),
            pltpu.VMEM((tiles, tile, half), f32),
            pltpu.VMEM((half, tokens), bf16),
            pltpu.VMEM((line, plane, half, quarter), f32),
            pltpu.VMEM((2, line, 2, 2, half // 2, quarter), bf16),
            pltpu.VMEM((2, line, 2, half // 2, quarter), bf16),
            pltpu.VMEM((2, line, half // 2, quarter), bf16),
            pltpu.VMEM((2, line, half // 2, quarter), bf16),
            pltpu.VMEM((line, half, quarter), bf16),
            pltpu.VMEM((line, half, quarter), bf16),
            pltpu.VMEM((plane, half, quarter), bf16),
            pltpu.VMEM((2, line, plane, half, quarter), bf16),
            pltpu.VMEM((rank, width), bf16),
            dma((11,)),
            dma((tiles, 2)),
            pltpu.SemaphoreType.REGULAR((2,)),
            dma((2, pieces)),
            dma((line - 1, pieces)),
            dma((line, pieces)),
            dma((line - 1, quarter_chunks, 2)),
            dma((line - 1, quarter_chunks, 2)),
            dma((line - 1, 2)),
            dma((line - 1, 2)),
            dma((tiles,)),
            dma((tiles,)),
            dma((2, line)),
            dma((2, line)),
            dma((2, line)),
            dma((2, line)),
            dma((line,)),
            dma((line,)),
            dma((plane - 1,)),
            dma((plane - 1,)),
            dma((line - 1,)),
            dma((line,)),
            dma((line, 2)),
            dma((line, 2)),
            dma((line, 2)),
            dma((line, 2)),
            dma((line,)),
            dma((line,)),
        ],
        compiler_params=pltpu.CompilerParams(
            collective_id=0, has_side_effects=True, vmem_limit_bytes=vmem_grant - held
        ),
    )(
        lambda_head,
        head_gain.reshape(1, -1),
        first_mix,
        second_mix,
        out_cotangent,
        basis,
        weight,
        first_moment,
        second_moment,
    )
    copied, new, step, first_new, second_new = pl.pallas_call(
        store_kernel,
        out_shape=tuple(jax.ShapeDtypeStruct(shape, kind) for shape, kind in shapes),
        in_specs=[on_chip] * 5,
        out_specs=(any_space,) * 5,
        scratch_shapes=[dma((5, 4))],
        compiler_params=pltpu.CompilerParams(vmem_limit_bytes=vmem_grant // 4),
    )(*(pltpu.with_memory_space_constraint(piece, pltpu.VMEM) for piece in fresh))
    return (new, copied, step, first_new, second_new)


def solution(mesh):
    line, plane, pair = (mesh.shape[name] for name in ("fs", "rep", "tp"))

    def chosen(*args):
        basis, first_moment = args[5], args[7]
        quarter_fits = first_moment.shape[0] % (plane * 128) == 0
        rows_fit = basis.shape[0] % (plane * 16) == 0 and basis.shape[0] % 64 == 0
        rank_fits = pair == 2 and first_moment.shape[1] % 128 == 0
        if line == 4 and plane == 4 and quarter_fits and rows_fit and rank_fits:
            return fast_body((line, plane), *args)
        return body(*args)

    return jax.shard_map(
        chosen,
        mesh=mesh,
        in_specs=(
            P(("fs", "rep"), "tp"),
            P(("fs", "rep"), "tp"),
            P("tp"),
            P(),
            P(("fs", "rep"), None),
            P("tp", None),
            P("tp", "fs"),
            P("fs", "tp"),
            P("fs", "tp"),
        ),
        out_specs=(P("tp", "fs"), P("tp", None), P("tp", "fs"), P("fs", "tp"), P("fs", "tp")),
        check_vma=False,
    )
```

```python
import functools

import jax
import jax.numpy as jnp
from jax import lax
from jax.experimental import pallas as pl
from jax.experimental.pallas import tpu as pltpu
from jax.sharding import PartitionSpec as P

MESH = pl.DeviceIdType.MESH

vmem_grant = 67043328
out_scale = 0.8
beta_first = 0.9
beta_second = 0.95
quarter_chunks = 4
extra_part = 10
own, across, turned, kept = -1, -2, -3, -4
plan = {
    16: ((own, 5),),
    17: ((own, 4), (0, 0),),
    4: ((0, 2),),
    6: ((0, 3),),
    7: ((0, 1), (1, 2),),
    8: ((kept,), (turned, 3), (1, 3), (0, 4),),
    11: (
        (1, 4),
        (1, 0),
        (2, 2),
        (turned, 1),
        (2, 3),
        (turned, 0),
        (turned, 2),
        (across, 1),
        (0, 5),
    ),
    12: ((1, 1), (2, 0), (across, 0), (1, 5), (2, 4), (2, 1), (across, 2),),
    15: ((2, 5),),
}


def head_output(first_piece, second_piece, lambdas, head_gain):
    token_count = first_piece.shape[0]
    head_width = head_gain.shape[0]
    head_count = lambdas.shape[0] // head_width
    mixture = first_piece.astype(jnp.float32) - lambdas[None, :] * second_piece.astype(jnp.float32)
    grouped = mixture.reshape(token_count, head_count, head_width)
    inverse = lax.rsqrt(jnp.mean(grouped * grouped, axis=-1, keepdims=True) + 1e-06)
    normed = grouped * inverse * head_gain[None, None, :] * out_scale
    return normed.reshape(token_count, head_count * head_width).astype(jnp.bfloat16)


def split_product(narrow, wide, numbers):
    upper = wide.astype(jnp.bfloat16)
    lower = (wide - upper.astype(jnp.float32)).astype(jnp.bfloat16)
    return lax.dot_general(
        narrow, upper, numbers, preferred_element_type=jnp.float32
    ) + lax.dot_general(narrow, lower, numbers, preferred_element_type=jnp.float32)


def body(
    first_mix,
    second_mix,
    lambda_head,
    head_gain,
    out_cotangent,
    basis,
    weight,
    first_moment,
    second_moment,
):
    lambdas = jnp.repeat(lambda_head, head_gain.shape[0])
    head_out = head_output(first_mix, second_mix, lambdas, head_gain)
    reduced = jnp.dot(head_out, basis, preferred_element_type=jnp.float32)
    proj_rows = lax.psum_scatter(
        split_product(out_cotangent, reduced, (((0,), (0,)), ((), ()))),
        "fs",
        scatter_dimension=0,
        tiled=True,
    )
    proj_rows = lax.psum_scatter(proj_rows, "tp", scatter_dimension=1, tiled=True)
    projected = lax.psum(proj_rows, "rep")
    first_new = beta_first * first_moment + (1.0 - beta_first) * projected
    second_new = beta_second * second_moment + (1.0 - beta_second) * projected * projected
    direction = first_new / (jnp.sqrt(second_new) + 1e-08)
    energy = lax.psum(jnp.sum(direction * direction), ("fs", "tp"))
    entries = direction.shape[0] * direction.shape[1] * lax.axis_size("fs") * lax.axis_size("tp")
    spread = jnp.sqrt(energy / entries)
    full_direction = lax.all_gather(direction, "tp", axis=1, tiled=True)
    step_out = split_product(basis, full_direction, (((1,), (1,)), ((), ()))) * (
        -1.0 / (spread + 1e-06)
    )
    weight_new = weight + step_out
    weight_copy = lax.all_gather(weight_new.astype(jnp.bfloat16), "fs", axis=1, tiled=True)
    return (weight_new, weight_copy, step_out, first_new, second_new)


def exchange_kernel(
    sizes,
    lambda_hbm,
    gain_hbm,
    first_hbm,
    second_hbm,
    cot_hbm,
    basis_hbm,
    weight_hbm,
    moment1_hbm,
    moment2_hbm,
    copy_ref,
    new_ref,
    step_ref,
    first_new_ref,
    second_new_ref,
    lambda_ref,
    gain_ref,
    first_v,
    second_v,
    cot_v,
    basis_v,
    weight_v,
    gathered_v,
    moment1_v,
    moment2_v,
    half_mine_v,
    half_send_v,
    half_recv_v,
    turned_v,
    mine_v,
    across_send_v,
    across_recv_v,
    joint_send_v,
    joint_recv_v,
    line_send_v,
    line_recv_v,
    projected_v,
    direction_v,
    joined_v,
    load_sem,
    tile_sem,
    ready_sem,
    wz_send,
    wf_send,
    wz_recv,
    wp_send,
    wp_recv,
    wr_send,
    wr_recv,
    half_send,
    half_recv,
    across_send,
    across_recv,
    joint_send,
    joint_recv,
    line_send,
    line_recv,
    proj_send,
    proj_recv,
    dz_send,
    dz_recv,
    dp_send,
    dp_recv,
    dr_send,
    dr_recv,
    dt_send,
    dt_recv,
):
    line, plane = sizes
    fs, rep, tp = lax.axis_index("fs"), lax.axis_index("rep"), lax.axis_index("tp")
    other = 1 - tp
    tokens, width = cot_v.shape
    half, quarter = direction_v.shape[-2:]
    values, shard = weight_v.shape
    quarter_rows = values // plane
    chunk = quarter_rows // quarter_chunks
    head_width = gain_ref.shape[1]
    heads = first_v.shape[1] // head_width
    tiles = tile_sem.shape[0]
    tile = tokens // tiles

    fast_side = rep + 1 - 2 * lax.rem(rep, 2)
    slow_side = lax.rem(rep + 2, 4)
    far_side = 3 - rep
    sides = (fast_side, slow_side)
    peers = (far_side, slow_side, fast_side, rep)

    near_source = 1 + lax.rem(fs, 2)
    last_source = jnp.where(fs < 2, 3, 0)
    sources = (near_source, 6 - fs - near_source - last_source, last_source)
    nexts = tuple(jnp.where(source < fs, fs + 1, fs - 1) for source in sources)
    goes_on = tuple((to >= 0) & (to < line) for to in nexts)

    def remote(source, target, send, recv, where):
        return pltpu.make_async_remote_copy(
            src_ref=source,
            dst_ref=target,
            send_sem=send,
            recv_sem=recv,
            device_id=where,
            device_id_type=MESH,
        )

    def rows_of(owner, start, size):
        return pl.ds(pl.multiple_of(owner * quarter_rows + start, 16), size)

    def weight_load(owner, at):
        rows = rows_of(owner, 0, quarter_rows)
        return pltpu.make_async_copy(weight_hbm.at[rows], weight_v.at[rows], load_sem.at[at])

    weight_loads = [weight_load(owner, at) for at, owner in enumerate((rep, far_side) + sides)]
    basis_loads = [
        pltpu.make_async_copy(
            basis_hbm.at[:, pl.ds(pl.multiple_of(side * half, half), half)],
            basis_v.at[:, pl.ds(at * half, half)],
            load_sem.at[4 + at],
        )
        for at, side in enumerate((tp, other))
    ]
    cot_load = pltpu.make_async_copy(cot_hbm, cot_v, load_sem.at[6])
    moment_loads = [
        pltpu.make_async_copy(moment1_hbm, moment1_v, load_sem.at[7]),
        pltpu.make_async_copy(moment2_hbm, moment2_v, load_sem.at[8]),
    ]
    small_loads = [
        pltpu.make_async_copy(lambda_hbm, lambda_ref, load_sem.at[9]),
        pltpu.make_async_copy(gain_hbm, gain_ref, load_sem.at[10]),
    ]
    weight_loads[0].start()
    for load in small_loads + basis_loads:
        load.start()
    tile_loads = []
    for t in range(tiles):
        rows = pl.ds(t * tile, tile)
        pieces = (
            pltpu.make_async_copy(first_hbm.at[rows], first_v.at[rows], tile_sem.at[t, 0]),
            pltpu.make_async_copy(second_hbm.at[rows], second_v.at[rows], tile_sem.at[t, 1]),
        )
        for piece in pieces:
            piece.start()
        tile_loads.append(pieces)

    near_line = ((fs < line - 1, fs + 1), (fs > 0, fs - 1))
    near_count = jnp.where((fs > 0) & (fs < line - 1), 2, 1)

    def greet_line(semaphore):
        for wanted, to in near_line:

            @pl.when(wanted)
            def _():
                pl.semaphore_signal(
                    semaphore, inc=1, device_id={"fs": to}, device_id_type=MESH
                )

    barrier = pltpu.get_barrier_semaphore()
    greet_line(barrier)
    for step in range(plane - 1):
        pl.semaphore_signal(
            barrier, inc=1, device_id={"rep": peers[step]}, device_id_type=MESH
        )
    pl.semaphore_signal(barrier, inc=1, device_id={"tp": other}, device_id_type=MESH)
    pl.semaphore_wait(barrier, near_count + plane)
    greet_line(ready_sem.at[0])

    sends = []
    guarded = []

    extra = quarter_rows * extra_part // 16
    rest = (quarter_rows - extra) // 2
    pieces = [(rep, c * chunk, chunk) for c in range(quarter_chunks)]
    pieces += [(far_side, c * (extra // 2), extra // 2) for c in range(2)]
    quarters = tuple(range(quarter_chunks))
    extras = (quarter_chunks, quarter_chunks + 1)

    def line_copy(source, c, send, to):
        here = gathered_v.at[source, rows_of(*pieces[c])]
        return remote(here, here, send, wz_recv.at[source, c], {"fs": to})

    def start_if(wanted, copy):
        @pl.when(wanted)
        def _():
            copy.start()

        guarded.append((wanted, copy))

    def narrow(c):
        rows = rows_of(*pieces[c])
        gathered_v[fs, rows] = weight_v[rows].astype(jnp.bfloat16)

    def send_own(c):
        start_if(fs < line - 1, line_copy(fs, c, wz_send.at[0, c], fs + 1))
        start_if(fs > 0, line_copy(fs, c, wz_send.at[1, c], fs - 1))

    def arrive(t, c):
        copy = line_copy(sources[t], c, wf_send.at[t, c], nexts[t])
        copy.wait_recv()
        start_if(goes_on[t], copy)
        if c in quarters:
            here = gathered_v.at[sources[t], rows_of(*pieces[c])]
            for side in range(2):
                copy = remote(
                    here,
                    here,
                    wp_send.at[t, c, side],
                    wp_recv.at[t, c, side],
                    {"rep": sides[side]},
                )
                copy.start()
                sends.append(copy)

    waited = set()

    def from_side(t, c, side):
        if (t, c, side) not in waited:
            waited.add((t, c, side))
            here = gathered_v.at[sources[t], rows_of(sides[side], c * chunk, chunk)]
            remote(
                here,
                here,
                wp_send.at[t, c, side],
                wp_recv.at[t, c, side],
                {"rep": sides[side]},
            ).wait_recv()

    def relay_copy(t, side, owner):
        here = gathered_v.at[sources[t], rows_of(owner, extra + side * rest, rest)]
        return remote(
            here, here, wr_send.at[t, side], wr_recv.at[t, side], {"rep": sides[1 - side]}
        )

    def relay(t):
        for side in range(2):
            start = extra + side * rest
            for c in range(start // chunk, -(-(start + rest) // chunk)):
                from_side(t, c, side)
            copy = relay_copy(t, side, sides[side])
            copy.start()
            sends.append(copy)

    def finish(t):
        for c in quarters:
            for side in range(2):
                from_side(t, c, side)
        for side in range(2):
            relay_copy(t, side, far_side).wait_recv()

    def weave(slot):
        for step in plan.get(slot, ()):
            if step[0] == own:
                send_own(step[1])
            elif step[0] == across:
                relay(step[1])
            elif step[0] == turned:
                relay_direction(step[1])
            elif step[0] == kept:
                spread_projected()
            else:
                arrive(*step)

    weight_loads[0].wait()
    cot_load.start()
    weight_loads[1].start()
    for load in moment_loads + weight_loads[2:]:
        load.start()
    for c in quarters:
        narrow(c)
        send_own(c)

    for load in basis_loads:
        load.wait()
    for load in small_loads:
        load.wait()
    gain = gain_ref[...] * out_scale
    half_copies = []

    def join_pair(t):
        half_copies[t].wait_recv()
        both = half_mine_v[t] + half_recv_v[t]
        turned_v[:, t * tile : (t + 1) * tile] = both.T.astype(jnp.bfloat16)

    for t in range(tiles):
        for piece in tile_loads[t]:
            piece.wait()
        rows = pl.ds(t * tile, tile)
        reduced = None
        for h in range(heads):
            lanes = pl.ds(h * head_width, head_width)
            mixture = first_v[rows, lanes].astype(jnp.float32) - lambda_ref[h] * second_v[
                rows, lanes
            ].astype(jnp.float32)
            inverse = lax.rsqrt(jnp.mean(mixture * mixture, axis=-1, keepdims=True) + 1e-06)
            normed = (mixture * inverse * gain).astype(jnp.bfloat16)
            term = jnp.dot(normed, basis_v[lanes, :], preferred_element_type=jnp.float32)
            reduced = term if reduced is None else reduced + term
        half_mine_v[t] = reduced[:, :half]
        half_send_v[t] = reduced[:, half:]
        copy = remote(
            half_send_v.at[t],
            half_recv_v.at[t],
            half_send.at[t],
            half_recv.at[t],
            {"tp": other},
        )
        copy.start()
        half_copies.append(copy)
        sends.append(copy)
        if t > 0:
            join_pair(t - 1)
        if t == tiles - 2:
            weave(0)
    pl.semaphore_wait(ready_sem.at[0], near_count)
    greet_line(ready_sem.at[1])
    weight_loads[1].wait()
    for c in extras:
        narrow(c)
    cot_load.wait()
    weave(16)
    join_pair(tiles - 1)
    weave(1)

    order = (2, 1, 3, 0)
    middle = half // 2
    halves = (pl.ds(0, middle), pl.ds(middle, middle))
    bits = (lax.rem(rep, 2), lax.div(rep, 2))
    across_copies = {}
    joint_copies = {}
    for ahead in order:
        at = lax.rem(fs + ahead, line)
        product = jnp.dot(
            turned_v[...],
            cot_v[:, pl.ds(pl.multiple_of(at * shard, shard), shard)],
            preferred_element_type=jnp.float32,
        )
        for part in range(plane):
            piece = product[:, part * quarter : (part + 1) * quarter]
            mine_v[ahead, part] = piece
            piece = piece.astype(jnp.bfloat16)
            across_send_v[0, ahead, part % 2, part // 2] = piece[:middle]
            across_send_v[1, ahead, part // 2, part % 2] = piece[middle:]
        for side in range(2):
            copy = remote(
                across_send_v.at[side, ahead, 1 - bits[side]],
                across_recv_v.at[side, ahead],
                across_send.at[side, ahead],
                across_recv.at[side, ahead],
                {"rep": sides[side]},
            )
            copy.start()
            across_copies[side, ahead] = copy
            sends.append(copy)
        if ahead == order[1]:
            weave(2)

    weave(3)
    for load in moment_loads:
        load.wait()
    my_quarter = pl.ds(pl.multiple_of(rep * quarter, quarter), quarter)
    moment1 = moment1_v[my_quarter].T
    moment2 = moment2_v[my_quarter].T

    for ahead in order:
        for side in range(2):
            across_copies[side, ahead].wait_recv()
            turn = 1 - side
            joint = (
                mine_v[ahead, sides[turn], halves[side]]
                + across_recv_v[side, ahead, 1 - bits[turn]].astype(jnp.float32)
            )
            joint_send_v[side, ahead] = joint.astype(jnp.bfloat16)
            copy = remote(
                joint_send_v.at[side, ahead],
                joint_recv_v.at[side, ahead],
                joint_send.at[side, ahead],
                joint_recv.at[side, ahead],
                {"rep": sides[turn]},
            )
            copy.start()
            joint_copies[side, ahead] = copy
            sends.append(copy)
        weave(17 + order.index(ahead))
    pl.semaphore_wait(ready_sem.at[1], near_count)
    line_copies = []
    for ahead in order:
        totals = []
        for side in range(2):
            joint_copies[side, ahead].wait_recv()
            totals.append(
                mine_v[ahead, rep, halves[side]]
                + across_recv_v[side, ahead, bits[1 - side]].astype(jnp.float32)
                + joint_recv_v[side, ahead].astype(jnp.float32)
            )
        total = jnp.concatenate(totals, axis=0)
        if ahead:
            line_send_v[ahead] = total.astype(jnp.bfloat16)
            copy = remote(
                line_send_v.at[ahead],
                line_recv_v.at[ahead],
                line_send.at[ahead],
                line_recv.at[ahead],
                {"fs": lax.rem(fs + ahead, line)},
            )
            copy.start()
            line_copies.append(copy)
            sends.append(copy)
        weave(4 + order.index(ahead))

    projected = total
    for copy, ahead in zip(line_copies, order):
        copy.wait_recv()
        projected = projected + line_recv_v[ahead].astype(jnp.float32)
    first_new = beta_first * moment1 + (1.0 - beta_first) * projected
    second_new = beta_second * moment2 + (1.0 - beta_second) * projected * projected
    direction = first_new / (jnp.sqrt(second_new) + 1e-08)
    direction_v[tp, fs, rep] = direction.astype(jnp.bfloat16)
    projected_v[rep] = projected.astype(jnp.bfloat16)

    def spread_line(source, to, at):
        here = direction_v.at[tp, source, rep]
        return remote(here, here, dz_send.at[at], dz_recv.at[source], {"fs": to})

    def spread_plane(at, source):
        for side in range(2):
            here = direction_v.at[tp, source, rep]
            copy = remote(
                here, here, dp_send.at[at, side], dp_recv.at[at, side], {"rep": sides[side]}
            )
            copy.start()
            sends.append(copy)

    def spread_relay_copy(at, side, owner):
        here = direction_v.at[tp, (sources + (fs,))[at], owner, halves[side]]
        return remote(
            here, here, dr_send.at[at, side], dr_recv.at[at, side], {"rep": sides[1 - side]}
        )

    def relay_direction(at):
        for side in range(2):
            here = direction_v.at[tp, (sources + (fs,))[at], sides[side]]
            remote(
                here, here, dp_send.at[at, side], dp_recv.at[at, side], {"rep": sides[side]}
            ).wait_recv()
            copy = spread_relay_copy(at, side, sides[side])
            copy.start()
            sends.append(copy)

    def to_pair(at, source):
        for side in range(2):
            spread_relay_copy(at, side, far_side).wait_recv()
        here = direction_v.at[tp, source]
        copy = remote(here, here, dt_send.at[at], dt_recv.at[at], {"tp": other})
        copy.start()
        sends.append(copy)

    for at, to in enumerate(sources):
        copy = spread_line(fs, to, at)
        copy.start()
        sends.append(copy)
    spread_plane(3, fs)
    proj_copies = []

    def spread_projected():
        for step in range(plane - 1):
            here = projected_v.at[rep]
            copy = remote(
                here, here, proj_send.at[step], proj_recv.at[step], {"rep": peers[step]}
            )
            copy.start()
            sends.append(copy)
            proj_copies.append(copy)

    weave(8)
    for at, source in enumerate(sources):
        spread_line(source, source, at).wait_recv()
        spread_plane(at, source)
        weave(9 + at)
    to_pair(3, fs)
    weave(12)
    for at, source in enumerate(sources):
        to_pair(at, source)
        weave(13 + at)

    for at, source in enumerate(sources + (fs,)):
        here = direction_v.at[other, source]
        remote(here, here, dt_send.at[at], dt_recv.at[at], {"tp": other}).wait_recv()
    energy = jnp.zeros((half, quarter), jnp.float32)
    for at in range(line):
        for part in range(plane):
            lanes = pl.ds((at * plane + part) * quarter, quarter)
            for side in range(2):
                wide = direction_v[side, at, part].astype(jnp.float32)
                energy += wide * wide
            joined_v[:half, lanes] = direction_v[tp, at, part]
            joined_v[half:, lanes] = direction_v[other, at, part]
    total = jnp.sum(jnp.sum(energy, axis=0, keepdims=True), axis=1, keepdims=True)
    spread = jnp.sqrt(total / (width * 2 * half))
    scale = -1.0 / (spread + 1e-06)
    weave(21)

    block = values // 4

    def step_block(at, rows):
        return (
            jnp.dot(
                basis_v[rows, :],
                joined_v[:, pl.ds(pl.multiple_of(at * shard, shard), shard)],
                preferred_element_type=jnp.float32,
            )
            * scale
        )

    def columns_of(at):
        return pl.ds(pl.multiple_of(at * shard, shard), shard)

    for load in weight_loads[2:]:
        load.wait()
    for b in range(4):
        rows = pl.ds(b * block, block)
        step = step_block(fs, rows)
        fresh = weight_v[rows, :] + step
        step_ref[rows, :] = step
        new_ref[rows, :] = fresh
        copy_ref[rows, columns_of(fs)] = fresh.astype(jnp.bfloat16)
    for copy in proj_copies:
        copy.wait_recv()
    for part in range(plane):
        rows = pl.ds(part * quarter, quarter)
        piece = projected_v[part].astype(jnp.float32).T
        first_new_ref[rows, :] = beta_first * moment1_v[rows, :] + (1.0 - beta_first) * piece
        second_new_ref[rows, :] = (
            beta_second * moment2_v[rows, :] + (1.0 - beta_second) * piece * piece
        )
    weave(22)
    for t, source in enumerate(sources):
        finish(t)
        for b in range(4):
            rows = pl.ds(b * block, block)
            copy_ref[rows, columns_of(source)] = (
                gathered_v[source, rows].astype(jnp.float32) + step_block(source, rows)
            ).astype(jnp.bfloat16)
        weave(23 + t)
    for copy in sends:
        copy.wait_send()
    for wanted, copy in guarded:

        @pl.when(wanted)
        def _():
            copy.wait_send()


def store_kernel(*refs):
    count = (len(refs) - 1) // 2
    sources, targets, store_sem = refs[:count], refs[count : 2 * count], refs[-1]
    copies = []
    for at in range(count):
        parts = store_sem.shape[1]
        rows = sources[at].shape[0] // parts
        for part in range(parts):
            here = pl.ds(part * rows, rows)
            copies.append(
                pltpu.make_async_copy(
                    sources[at].at[here], targets[at].at[here], store_sem.at[at, part]
                )
            )
    for copy in copies:
        copy.start()
    for copy in copies:
        copy.wait()


def fast_body(
    sizes,
    first_mix,
    second_mix,
    lambda_head,
    head_gain,
    out_cotangent,
    basis,
    weight,
    first_moment,
    second_moment,
):
    line, plane = sizes
    tokens, width = out_cotangent.shape
    values, rank = basis.shape
    shard, half = first_moment.shape
    quarter = shard // plane
    tile = 256 if tokens % 256 == 0 else tokens
    tiles = tokens // tile
    pieces = quarter_chunks + 2
    any_space = pl.BlockSpec(memory_space=pl.ANY)
    on_chip = pl.BlockSpec(memory_space=pltpu.VMEM)
    dma = pltpu.SemaphoreType.DMA
    f32, bf16 = jnp.float32, jnp.bfloat16
    shapes = (
        ((values, width), bf16),
        (weight.shape, f32),
        (weight.shape, f32),
        (first_moment.shape, f32),
        (first_moment.shape, f32),
    )
    held = sum(jnp.dtype(kind).itemsize * shape[0] * shape[1] for shape, kind in shapes)
    fresh = pl.pallas_call(
        functools.partial(exchange_kernel, sizes),
        out_shape=tuple(pltpu.VMEM(shape, kind) for shape, kind in shapes),
        in_specs=[any_space] * 9,
        out_specs=(on_chip,) * 5,
        scratch_shapes=[
            pltpu.SMEM(lambda_head.shape, f32),
            pltpu.VMEM((1, head_gain.shape[0]), f32),
            pltpu.VMEM(first_mix.shape, bf16),
            pltpu.VMEM(second_mix.shape, bf16),
            pltpu.VMEM(out_cotangent.shape, bf16),
            pltpu.VMEM(basis.shape, bf16),
            pltpu.VMEM(weight.shape, f32),
            pltpu.VMEM((line, values, shard), bf16),
            pltpu.VMEM(first_moment.shape, f32),
            pltpu.VMEM(first_moment.shape, f32),
            pltpu.VMEM((tiles, tile, half), f32),
            pltpu.VMEM((tiles, tile, half), f32),
            pltpu.VMEM((tiles, tile, half), f32),
            pltpu.VMEM((half, tokens), bf16),
            pltpu.VMEM((line, plane, half, quarter), f32),
            pltpu.VMEM((2, line, 2, 2, half // 2, quarter), bf16),
            pltpu.VMEM((2, line, 2, half // 2, quarter), bf16),
            pltpu.VMEM((2, line, half // 2, quarter), bf16),
            pltpu.VMEM((2, line, half // 2, quarter), bf16),
            pltpu.VMEM((line, half, quarter), bf16),
            pltpu.VMEM((line, half, quarter), bf16),
            pltpu.VMEM((plane, half, quarter), bf16),
            pltpu.VMEM((2, line, plane, half, quarter), bf16),
            pltpu.VMEM((rank, width), bf16),
            dma((11,)),
            dma((tiles, 2)),
            pltpu.SemaphoreType.REGULAR((2,)),
            dma((2, pieces)),
            dma((line - 1, pieces)),
            dma((line, pieces)),
            dma((line - 1, quarter_chunks, 2)),
            dma((line - 1, quarter_chunks, 2)),
            dma((line - 1, 2)),
            dma((line - 1, 2)),
            dma((tiles,)),
            dma((tiles,)),
            dma((2, line)),
            dma((2, line)),
            dma((2, line)),
            dma((2, line)),
            dma((line,)),
            dma((line,)),
            dma((plane - 1,)),
            dma((plane - 1,)),
            dma((line - 1,)),
            dma((line,)),
            dma((line, 2)),
            dma((line, 2)),
            dma((line, 2)),
            dma((line, 2)),
            dma((line,)),
            dma((line,)),
        ],
        compiler_params=pltpu.CompilerParams(
            collective_id=0, has_side_effects=True, vmem_limit_bytes=vmem_grant - held
        ),
    )(
        lambda_head,
        head_gain.reshape(1, -1),
        first_mix,
        second_mix,
        out_cotangent,
        basis,
        weight,
        first_moment,
        second_moment,
    )
    copied, new, step, first_new, second_new = pl.pallas_call(
        store_kernel,
        out_shape=tuple(jax.ShapeDtypeStruct(shape, kind) for shape, kind in shapes),
        in_specs=[on_chip] * 5,
        out_specs=(any_space,) * 5,
        scratch_shapes=[dma((5, 1))],
        compiler_params=pltpu.CompilerParams(vmem_limit_bytes=vmem_grant // 4),
    )(*(pltpu.with_memory_space_constraint(piece, pltpu.VMEM) for piece in fresh))
    return (new, copied, step, first_new, second_new)


def solution(mesh):
    line, plane, pair = (mesh.shape[name] for name in ("fs", "rep", "tp"))

    def chosen(*args):
        basis, first_moment = args[5], args[7]
        quarter_fits = first_moment.shape[0] % (plane * 128) == 0
        rows_fit = basis.shape[0] % (plane * 16) == 0 and basis.shape[0] % 64 == 0
        rank_fits = pair == 2 and first_moment.shape[1] % 128 == 0
        if line == 4 and plane == 4 and quarter_fits and rows_fit and rank_fits:
            return fast_body((line, plane), *args)
        return body(*args)

    return jax.shard_map(
        chosen,
        mesh=mesh,
        in_specs=(
            P(("fs", "rep"), "tp"),
            P(("fs", "rep"), "tp"),
            P("tp"),
            P(),
            P(("fs", "rep"), None),
            P("tp", None),
            P("tp", "fs"),
            P("fs", "tp"),
            P("fs", "tp"),
        ),
        out_specs=(P("tp", "fs"), P("tp", None), P("tp", "fs"), P("fs", "tp"), P("fs", "tp")),
        check_vma=False,
    )
```

```python
import functools

import jax
import jax.numpy as jnp
from jax import lax
from jax.experimental import pallas as pl
from jax.experimental.pallas import tpu as pltpu
from jax.sharding import PartitionSpec as P

MESH = pl.DeviceIdType.MESH

vmem_grant = 67043328
out_scale = 0.8
beta_first = 0.9
beta_second = 0.95
quarter_chunks = 4
extra_part = 10
own, across, turned = -1, -2, -3
plan = {
    16: ((own, 5),),
    17: ((own, 4), (0, 0),),
    4: ((0, 2),),
    6: ((0, 3),),
    7: ((0, 1), (1, 2),),
    8: ((0, 4), (1, 0), (1, 3),),
    10: ((turned, 3),),
    11: ((1, 4), (2, 2), (turned, 1), (2, 3), (turned, 0), (turned, 2), (across, 1), (0, 5),),
    12: ((1, 1), (2, 0), (across, 0), (1, 5), (2, 4), (2, 1), (across, 2),),
    15: ((2, 5),),
}


def head_output(first_piece, second_piece, lambdas, head_gain):
    token_count = first_piece.shape[0]
    head_width = head_gain.shape[0]
    head_count = lambdas.shape[0] // head_width
    mixture = first_piece.astype(jnp.float32) - lambdas[None, :] * second_piece.astype(jnp.float32)
    grouped = mixture.reshape(token_count, head_count, head_width)
    inverse = lax.rsqrt(jnp.mean(grouped * grouped, axis=-1, keepdims=True) + 1e-06)
    normed = grouped * inverse * head_gain[None, None, :] * out_scale
    return normed.reshape(token_count, head_count * head_width).astype(jnp.bfloat16)


def split_product(narrow, wide, numbers):
    upper = wide.astype(jnp.bfloat16)
    lower = (wide - upper.astype(jnp.float32)).astype(jnp.bfloat16)
    return lax.dot_general(
        narrow, upper, numbers, preferred_element_type=jnp.float32
    ) + lax.dot_general(narrow, lower, numbers, preferred_element_type=jnp.float32)


def body(
    first_mix,
    second_mix,
    lambda_head,
    head_gain,
    out_cotangent,
    basis,
    weight,
    first_moment,
    second_moment,
):
    lambdas = jnp.repeat(lambda_head, head_gain.shape[0])
    head_out = head_output(first_mix, second_mix, lambdas, head_gain)
    reduced = jnp.dot(head_out, basis, preferred_element_type=jnp.float32)
    proj_rows = lax.psum_scatter(
        split_product(out_cotangent, reduced, (((0,), (0,)), ((), ()))),
        "fs",
        scatter_dimension=0,
        tiled=True,
    )
    proj_rows = lax.psum_scatter(proj_rows, "tp", scatter_dimension=1, tiled=True)
    projected = lax.psum(proj_rows, "rep")
    first_new = beta_first * first_moment + (1.0 - beta_first) * projected
    second_new = beta_second * second_moment + (1.0 - beta_second) * projected * projected
    direction = first_new / (jnp.sqrt(second_new) + 1e-08)
    energy = lax.psum(jnp.sum(direction * direction), ("fs", "tp"))
    entries = direction.shape[0] * direction.shape[1] * lax.axis_size("fs") * lax.axis_size("tp")
    spread = jnp.sqrt(energy / entries)
    full_direction = lax.all_gather(direction, "tp", axis=1, tiled=True)
    step_out = split_product(basis, full_direction, (((1,), (1,)), ((), ()))) * (
        -1.0 / (spread + 1e-06)
    )
    weight_new = weight + step_out
    weight_copy = lax.all_gather(weight_new.astype(jnp.bfloat16), "fs", axis=1, tiled=True)
    return (weight_new, weight_copy, step_out, first_new, second_new)


def exchange_kernel(
    sizes,
    lambda_hbm,
    gain_hbm,
    first_hbm,
    second_hbm,
    cot_hbm,
    basis_hbm,
    weight_hbm,
    moment1_hbm,
    moment2_hbm,
    copy_ref,
    new_ref,
    step_ref,
    first_new_ref,
    second_new_ref,
    lambda_ref,
    gain_ref,
    first_v,
    second_v,
    cot_v,
    basis_v,
    weight_v,
    gathered_v,
    moment1_v,
    moment2_v,
    half_mine_v,
    half_send_v,
    half_recv_v,
    turned_v,
    mine_v,
    across_send_v,
    across_recv_v,
    joint_send_v,
    joint_recv_v,
    line_send_v,
    line_recv_v,
    projected_v,
    direction_v,
    joined_v,
    load_sem,
    tile_sem,
    ready_sem,
    wz_send,
    wf_send,
    wz_recv,
    wp_send,
    wp_recv,
    wr_send,
    wr_recv,
    half_send,
    half_recv,
    across_send,
    across_recv,
    joint_send,
    joint_recv,
    line_send,
    line_recv,
    dz_send,
    dz_recv,
    dp_send,
    dp_recv,
    dr_send,
    dr_recv,
    dt_send,
    dt_recv,
):
    line, plane = sizes
    fs, rep, tp = lax.axis_index("fs"), lax.axis_index("rep"), lax.axis_index("tp")
    other = 1 - tp
    tokens, width = cot_v.shape
    half, quarter = direction_v.shape[-2:]
    values, shard = weight_v.shape
    quarter_rows = values // plane
    chunk = quarter_rows // quarter_chunks
    head_width = gain_ref.shape[1]
    heads = first_v.shape[1] // head_width
    tiles = tile_sem.shape[0]
    tile = tokens // tiles

    fast_side = rep + 1 - 2 * lax.rem(rep, 2)
    slow_side = lax.rem(rep + 2, 4)
    far_side = 3 - rep
    sides = (fast_side, slow_side)
    peers = (far_side, slow_side, fast_side, rep)

    near_source = 1 + lax.rem(fs, 2)
    last_source = jnp.where(fs < 2, 3, 0)
    sources = (near_source, 6 - fs - near_source - last_source, last_source)
    nexts = tuple(jnp.where(source < fs, fs + 1, fs - 1) for source in sources)
    goes_on = tuple((to >= 0) & (to < line) for to in nexts)

    def remote(source, target, send, recv, where):
        return pltpu.make_async_remote_copy(
            src_ref=source,
            dst_ref=target,
            send_sem=send,
            recv_sem=recv,
            device_id=where,
            device_id_type=MESH,
        )

    def rows_of(owner, start, size):
        return pl.ds(pl.multiple_of(owner * quarter_rows + start, 16), size)

    def weight_load(owner, at):
        rows = rows_of(owner, 0, quarter_rows)
        return pltpu.make_async_copy(weight_hbm.at[rows], weight_v.at[rows], load_sem.at[at])

    weight_loads = [weight_load(owner, at) for at, owner in enumerate((rep, far_side) + sides)]
    basis_loads = [
        pltpu.make_async_copy(
            basis_hbm.at[:, pl.ds(pl.multiple_of(side * half, half), half)],
            basis_v.at[:, pl.ds(at * half, half)],
            load_sem.at[4 + at],
        )
        for at, side in enumerate((tp, other))
    ]
    cot_load = pltpu.make_async_copy(cot_hbm, cot_v, load_sem.at[6])
    moment_loads = [
        pltpu.make_async_copy(moment1_hbm, moment1_v, load_sem.at[7]),
        pltpu.make_async_copy(moment2_hbm, moment2_v, load_sem.at[8]),
    ]
    small_loads = [
        pltpu.make_async_copy(lambda_hbm, lambda_ref, load_sem.at[9]),
        pltpu.make_async_copy(gain_hbm, gain_ref, load_sem.at[10]),
    ]
    weight_loads[0].start()
    for load in small_loads + basis_loads:
        load.start()
    tile_loads = []
    for t in range(tiles):
        rows = pl.ds(t * tile, tile)
        pieces = (
            pltpu.make_async_copy(first_hbm.at[rows], first_v.at[rows], tile_sem.at[t, 0]),
            pltpu.make_async_copy(second_hbm.at[rows], second_v.at[rows], tile_sem.at[t, 1]),
        )
        for piece in pieces:
            piece.start()
        tile_loads.append(pieces)

    near_line = ((fs < line - 1, fs + 1), (fs > 0, fs - 1))
    near_count = jnp.where((fs > 0) & (fs < line - 1), 2, 1)

    def greet_line(semaphore):
        for wanted, to in near_line:

            @pl.when(wanted)
            def _():
                pl.semaphore_signal(
                    semaphore, inc=1, device_id={"fs": to}, device_id_type=MESH
                )

    barrier = pltpu.get_barrier_semaphore()
    greet_line(barrier)
    for step in range(plane - 1):
        pl.semaphore_signal(
            barrier, inc=1, device_id={"rep": peers[step]}, device_id_type=MESH
        )
    pl.semaphore_signal(barrier, inc=1, device_id={"tp": other}, device_id_type=MESH)
    pl.semaphore_wait(barrier, near_count + plane)
    greet_line(ready_sem.at[0])

    sends = []
    guarded = []

    extra = quarter_rows * extra_part // 16
    rest = (quarter_rows - extra) // 2
    pieces = [(rep, c * chunk, chunk) for c in range(quarter_chunks)]
    pieces += [(far_side, c * (extra // 2), extra // 2) for c in range(2)]
    quarters = tuple(range(quarter_chunks))
    extras = (quarter_chunks, quarter_chunks + 1)

    def line_copy(source, c, send, to):
        here = gathered_v.at[source, rows_of(*pieces[c])]
        return remote(here, here, send, wz_recv.at[source, c], {"fs": to})

    def start_if(wanted, copy):
        @pl.when(wanted)
        def _():
            copy.start()

        guarded.append((wanted, copy))

    def narrow(c):
        rows = rows_of(*pieces[c])
        gathered_v[fs, rows] = weight_v[rows].astype(jnp.bfloat16)

    def send_own(c):
        start_if(fs < line - 1, line_copy(fs, c, wz_send.at[0, c], fs + 1))
        start_if(fs > 0, line_copy(fs, c, wz_send.at[1, c], fs - 1))

    def arrive(t, c):
        copy = line_copy(sources[t], c, wf_send.at[t, c], nexts[t])
        copy.wait_recv()
        start_if(goes_on[t], copy)
        if c in quarters:
            here = gathered_v.at[sources[t], rows_of(*pieces[c])]
            for side in range(2):
                copy = remote(
                    here,
                    here,
                    wp_send.at[t, c, side],
                    wp_recv.at[t, c, side],
                    {"rep": sides[side]},
                )
                copy.start()
                sends.append(copy)

    waited = set()

    def from_side(t, c, side):
        if (t, c, side) not in waited:
            waited.add((t, c, side))
            here = gathered_v.at[sources[t], rows_of(sides[side], c * chunk, chunk)]
            remote(
                here,
                here,
                wp_send.at[t, c, side],
                wp_recv.at[t, c, side],
                {"rep": sides[side]},
            ).wait_recv()

    def relay_copy(t, side, owner):
        here = gathered_v.at[sources[t], rows_of(owner, extra + side * rest, rest)]
        return remote(
            here, here, wr_send.at[t, side], wr_recv.at[t, side], {"rep": sides[1 - side]}
        )

    def relay(t):
        for side in range(2):
            start = extra + side * rest
            for c in range(start // chunk, -(-(start + rest) // chunk)):
                from_side(t, c, side)
            copy = relay_copy(t, side, sides[side])
            copy.start()
            sends.append(copy)

    def finish(t):
        for c in quarters:
            for side in range(2):
                from_side(t, c, side)
        for side in range(2):
            relay_copy(t, side, far_side).wait_recv()

    def weave(slot):
        for step in plan.get(slot, ()):
            if step[0] == own:
                send_own(step[1])
            elif step[0] == across:
                relay(step[1])
            elif step[0] == turned:
                relay_direction(step[1])
            else:
                arrive(*step)

    weight_loads[0].wait()
    cot_load.start()
    weight_loads[1].start()
    for load in moment_loads + weight_loads[2:]:
        load.start()
    for c in quarters:
        narrow(c)
        send_own(c)

    for load in basis_loads:
        load.wait()
    for load in small_loads:
        load.wait()
    gain = gain_ref[...] * out_scale
    half_copies = []

    def join_pair(t):
        half_copies[t].wait_recv()
        both = half_mine_v[t] + half_recv_v[t]
        turned_v[:, t * tile : (t + 1) * tile] = both.T.astype(jnp.bfloat16)

    for t in range(tiles):
        for piece in tile_loads[t]:
            piece.wait()
        rows = pl.ds(t * tile, tile)
        reduced = None
        for h in range(heads):
            lanes = pl.ds(h * head_width, head_width)
            mixture = first_v[rows, lanes].astype(jnp.float32) - lambda_ref[h] * second_v[
                rows, lanes
            ].astype(jnp.float32)
            inverse = lax.rsqrt(jnp.mean(mixture * mixture, axis=-1, keepdims=True) + 1e-06)
            normed = (mixture * inverse * gain).astype(jnp.bfloat16)
            term = jnp.dot(normed, basis_v[lanes, :], preferred_element_type=jnp.float32)
            reduced = term if reduced is None else reduced + term
        half_mine_v[t] = reduced[:, :half]
        half_send_v[t] = reduced[:, half:]
        copy = remote(
            half_send_v.at[t],
            half_recv_v.at[t],
            half_send.at[t],
            half_recv.at[t],
            {"tp": other},
        )
        copy.start()
        half_copies.append(copy)
        sends.append(copy)
        if t > 0:
            join_pair(t - 1)
        if t == tiles - 2:
            weave(0)
    pl.semaphore_wait(ready_sem.at[0], near_count)
    greet_line(ready_sem.at[1])
    weight_loads[1].wait()
    for c in extras:
        narrow(c)
    cot_load.wait()
    weave(16)
    join_pair(tiles - 1)
    weave(1)

    order = (2, 1, 3, 0)
    middle = half // 2
    halves = (pl.ds(0, middle), pl.ds(middle, middle))
    bits = (lax.rem(rep, 2), lax.div(rep, 2))
    across_copies = {}
    joint_copies = {}
    for ahead in order:
        at = lax.rem(fs + ahead, line)
        product = jnp.dot(
            turned_v[...],
            cot_v[:, pl.ds(pl.multiple_of(at * shard, shard), shard)],
            preferred_element_type=jnp.float32,
        )
        for part in range(plane):
            piece = product[:, part * quarter : (part + 1) * quarter]
            mine_v[ahead, part] = piece
            piece = piece.astype(jnp.bfloat16)
            across_send_v[0, ahead, part % 2, part // 2] = piece[:middle]
            across_send_v[1, ahead, part // 2, part % 2] = piece[middle:]
        for side in range(2):
            copy = remote(
                across_send_v.at[side, ahead, 1 - bits[side]],
                across_recv_v.at[side, ahead],
                across_send.at[side, ahead],
                across_recv.at[side, ahead],
                {"rep": sides[side]},
            )
            copy.start()
            across_copies[side, ahead] = copy
            sends.append(copy)
        if ahead == order[1]:
            weave(2)

    weave(3)
    for load in moment_loads:
        load.wait()
    my_quarter = pl.ds(pl.multiple_of(rep * quarter, quarter), quarter)
    moment1 = moment1_v[my_quarter].T
    moment2 = moment2_v[my_quarter].T

    for ahead in order:
        for side in range(2):
            across_copies[side, ahead].wait_recv()
            turn = 1 - side
            joint = (
                mine_v[ahead, sides[turn], halves[side]]
                + across_recv_v[side, ahead, 1 - bits[turn]].astype(jnp.float32)
            )
            joint_send_v[side, ahead] = joint.astype(jnp.bfloat16)
            copy = remote(
                joint_send_v.at[side, ahead],
                joint_recv_v.at[side, ahead],
                joint_send.at[side, ahead],
                joint_recv.at[side, ahead],
                {"rep": sides[turn]},
            )
            copy.start()
            joint_copies[side, ahead] = copy
            sends.append(copy)
        weave(17 + order.index(ahead))
    pl.semaphore_wait(ready_sem.at[1], near_count)
    line_copies = []
    for ahead in order:
        totals = []
        for side in range(2):
            joint_copies[side, ahead].wait_recv()
            totals.append(
                mine_v[ahead, rep, halves[side]]
                + across_recv_v[side, ahead, bits[1 - side]].astype(jnp.float32)
                + joint_recv_v[side, ahead].astype(jnp.float32)
            )
        total = jnp.concatenate(totals, axis=0)
        if ahead:
            line_send_v[ahead] = total.astype(jnp.bfloat16)
            copy = remote(
                line_send_v.at[ahead],
                line_recv_v.at[ahead],
                line_send.at[ahead],
                line_recv.at[ahead],
                {"fs": lax.rem(fs + ahead, line)},
            )
            copy.start()
            line_copies.append(copy)
            sends.append(copy)
        weave(4 + order.index(ahead))

    projected = total
    for copy, ahead in zip(line_copies, order):
        copy.wait_recv()
        projected = projected + line_recv_v[ahead].astype(jnp.float32)
    projected_v[rep] = projected.astype(jnp.bfloat16)

    def settle(part, moment1, moment2):
        wide = projected_v[part].astype(jnp.float32)
        first_new = beta_first * moment1 + (1.0 - beta_first) * wide
        second_new = beta_second * moment2 + (1.0 - beta_second) * wide * wide
        direction = first_new / (jnp.sqrt(second_new) + 1e-08)
        direction_v[tp, fs, part] = direction.astype(jnp.bfloat16)

    settle(rep, moment1, moment2)

    def spread_line(source, to, at):
        here = direction_v.at[tp, source, rep]
        return remote(here, here, dz_send.at[at], dz_recv.at[source], {"fs": to})

    def piece_of(at, *where):
        if at == line - 1:
            return projected_v.at[where]
        return direction_v.at[(tp, sources[at]) + where]

    def spread_plane(at):
        for side in range(2):
            here = piece_of(at, rep)
            copy = remote(
                here, here, dp_send.at[at, side], dp_recv.at[at, side], {"rep": sides[side]}
            )
            copy.start()
            sends.append(copy)

    def spread_relay_copy(at, side, owner):
        here = piece_of(at, owner, halves[side])
        return remote(
            here, here, dr_send.at[at, side], dr_recv.at[at, side], {"rep": sides[1 - side]}
        )

    def relay_direction(at):
        for side in range(2):
            here = piece_of(at, sides[side])
            remote(
                here, here, dp_send.at[at, side], dp_recv.at[at, side], {"rep": sides[side]}
            ).wait_recv()
            copy = spread_relay_copy(at, side, sides[side])
            copy.start()
            sends.append(copy)

    def to_pair(at, source):
        for side in range(2):
            spread_relay_copy(at, side, far_side).wait_recv()
        if at == line - 1:
            for part in peers[:-1]:
                rows = pl.ds(pl.multiple_of(part * quarter, quarter), quarter)
                settle(part, moment1_v[rows].T, moment2_v[rows].T)
        here = direction_v.at[tp, source]
        copy = remote(here, here, dt_send.at[at], dt_recv.at[at], {"tp": other})
        copy.start()
        sends.append(copy)

    for at, to in enumerate(sources):
        copy = spread_line(fs, to, at)
        copy.start()
        sends.append(copy)
    spread_plane(3)
    weave(8)
    for at, source in enumerate(sources):
        spread_line(source, source, at).wait_recv()
        spread_plane(at)
        weave(9 + at)
    to_pair(3, fs)
    weave(12)
    for at, source in enumerate(sources):
        to_pair(at, source)
        weave(13 + at)

    for at, source in enumerate(sources + (fs,)):
        here = direction_v.at[other, source]
        remote(here, here, dt_send.at[at], dt_recv.at[at], {"tp": other}).wait_recv()
    energy = jnp.zeros((half, quarter), jnp.float32)
    for at in range(line):
        for part in range(plane):
            lanes = pl.ds((at * plane + part) * quarter, quarter)
            for side in range(2):
                wide = direction_v[side, at, part].astype(jnp.float32)
                energy += wide * wide
            joined_v[:half, lanes] = direction_v[tp, at, part]
            joined_v[half:, lanes] = direction_v[other, at, part]
    total = jnp.sum(jnp.sum(energy, axis=0, keepdims=True), axis=1, keepdims=True)
    spread = jnp.sqrt(total / (width * 2 * half))
    scale = -1.0 / (spread + 1e-06)
    weave(21)

    block = values // 4

    def step_block(at, rows):
        return (
            jnp.dot(
                basis_v[rows, :],
                joined_v[:, pl.ds(pl.multiple_of(at * shard, shard), shard)],
                preferred_element_type=jnp.float32,
            )
            * scale
        )

    def columns_of(at):
        return pl.ds(pl.multiple_of(at * shard, shard), shard)

    for load in weight_loads[2:]:
        load.wait()
    for b in range(4):
        rows = pl.ds(b * block, block)
        step = step_block(fs, rows)
        fresh = weight_v[rows, :] + step
        step_ref[rows, :] = step
        new_ref[rows, :] = fresh
        copy_ref[rows, columns_of(fs)] = fresh.astype(jnp.bfloat16)
    for part in range(plane):
        rows = pl.ds(part * quarter, quarter)
        piece = projected_v[part].astype(jnp.float32).T
        first_new_ref[rows, :] = beta_first * moment1_v[rows, :] + (1.0 - beta_first) * piece
        second_new_ref[rows, :] = (
            beta_second * moment2_v[rows, :] + (1.0 - beta_second) * piece * piece
        )
    weave(22)
    for t, source in enumerate(sources):
        finish(t)
        for b in range(4):
            rows = pl.ds(b * block, block)
            copy_ref[rows, columns_of(source)] = (
                gathered_v[source, rows].astype(jnp.float32) + step_block(source, rows)
            ).astype(jnp.bfloat16)
        weave(23 + t)
    for copy in sends:
        copy.wait_send()
    for wanted, copy in guarded:

        @pl.when(wanted)
        def _():
            copy.wait_send()


def store_kernel(*refs):
    count = (len(refs) - 1) // 2
    sources, targets, store_sem = refs[:count], refs[count : 2 * count], refs[-1]
    copies = []
    for at in range(count):
        parts = store_sem.shape[1]
        rows = sources[at].shape[0] // parts
        for part in range(parts):
            here = pl.ds(part * rows, rows)
            copies.append(
                pltpu.make_async_copy(
                    sources[at].at[here], targets[at].at[here], store_sem.at[at, part]
                )
            )
    for copy in copies:
        copy.start()
    for copy in copies:
        copy.wait()


def fast_body(
    sizes,
    first_mix,
    second_mix,
    lambda_head,
    head_gain,
    out_cotangent,
    basis,
    weight,
    first_moment,
    second_moment,
):
    line, plane = sizes
    tokens, width = out_cotangent.shape
    values, rank = basis.shape
    shard, half = first_moment.shape
    quarter = shard // plane
    tile = 256 if tokens % 256 == 0 else tokens
    tiles = tokens // tile
    pieces = quarter_chunks + 2
    any_space = pl.BlockSpec(memory_space=pl.ANY)
    on_chip = pl.BlockSpec(memory_space=pltpu.VMEM)
    dma = pltpu.SemaphoreType.DMA
    f32, bf16 = jnp.float32, jnp.bfloat16
    shapes = (
        ((values, width), bf16),
        (weight.shape, f32),
        (weight.shape, f32),
        (first_moment.shape, f32),
        (first_moment.shape, f32),
    )
    held = sum(jnp.dtype(kind).itemsize * shape[0] * shape[1] for shape, kind in shapes)
    fresh = pl.pallas_call(
        functools.partial(exchange_kernel, sizes),
        out_shape=tuple(pltpu.VMEM(shape, kind) for shape, kind in shapes),
        in_specs=[any_space] * 9,
        out_specs=(on_chip,) * 5,
        scratch_shapes=[
            pltpu.SMEM(lambda_head.shape, f32),
            pltpu.VMEM((1, head_gain.shape[0]), f32),
            pltpu.VMEM(first_mix.shape, bf16),
            pltpu.VMEM(second_mix.shape, bf16),
            pltpu.VMEM(out_cotangent.shape, bf16),
            pltpu.VMEM(basis.shape, bf16),
            pltpu.VMEM(weight.shape, f32),
            pltpu.VMEM((line, values, shard), bf16),
            pltpu.VMEM(first_moment.shape, f32),
            pltpu.VMEM(first_moment.shape, f32),
            pltpu.VMEM((tiles, tile, half), f32),
            pltpu.VMEM((tiles, tile, half), f32),
            pltpu.VMEM((tiles, tile, half), f32),
            pltpu.VMEM((half, tokens), bf16),
            pltpu.VMEM((line, plane, half, quarter), f32),
            pltpu.VMEM((2, line, 2, 2, half // 2, quarter), bf16),
            pltpu.VMEM((2, line, 2, half // 2, quarter), bf16),
            pltpu.VMEM((2, line, half // 2, quarter), bf16),
            pltpu.VMEM((2, line, half // 2, quarter), bf16),
            pltpu.VMEM((line, half, quarter), bf16),
            pltpu.VMEM((line, half, quarter), bf16),
            pltpu.VMEM((plane, half, quarter), bf16),
            pltpu.VMEM((2, line, plane, half, quarter), bf16),
            pltpu.VMEM((rank, width), bf16),
            dma((11,)),
            dma((tiles, 2)),
            pltpu.SemaphoreType.REGULAR((2,)),
            dma((2, pieces)),
            dma((line - 1, pieces)),
            dma((line, pieces)),
            dma((line - 1, quarter_chunks, 2)),
            dma((line - 1, quarter_chunks, 2)),
            dma((line - 1, 2)),
            dma((line - 1, 2)),
            dma((tiles,)),
            dma((tiles,)),
            dma((2, line)),
            dma((2, line)),
            dma((2, line)),
            dma((2, line)),
            dma((line,)),
            dma((line,)),
            dma((line - 1,)),
            dma((line,)),
            dma((line, 2)),
            dma((line, 2)),
            dma((line, 2)),
            dma((line, 2)),
            dma((line,)),
            dma((line,)),
        ],
        compiler_params=pltpu.CompilerParams(
            collective_id=0, has_side_effects=True, vmem_limit_bytes=vmem_grant - held
        ),
    )(
        lambda_head,
        head_gain.reshape(1, -1),
        first_mix,
        second_mix,
        out_cotangent,
        basis,
        weight,
        first_moment,
        second_moment,
    )
    copied, new, step, first_new, second_new = pl.pallas_call(
        store_kernel,
        out_shape=tuple(jax.ShapeDtypeStruct(shape, kind) for shape, kind in shapes),
        in_specs=[on_chip] * 5,
        out_specs=(any_space,) * 5,
        scratch_shapes=[dma((5, 1))],
        compiler_params=pltpu.CompilerParams(vmem_limit_bytes=vmem_grant // 4),
    )(*(pltpu.with_memory_space_constraint(piece, pltpu.VMEM) for piece in fresh))
    return (new, copied, step, first_new, second_new)


def solution(mesh):
    line, plane, pair = (mesh.shape[name] for name in ("fs", "rep", "tp"))

    def chosen(*args):
        basis, first_moment = args[5], args[7]
        quarter_fits = first_moment.shape[0] % (plane * 128) == 0
        rows_fit = basis.shape[0] % (plane * 16) == 0 and basis.shape[0] % 64 == 0
        rank_fits = pair == 2 and first_moment.shape[1] % 128 == 0
        if line == 4 and plane == 4 and quarter_fits and rows_fit and rank_fits:
            return fast_body((line, plane), *args)
        return body(*args)

    return jax.shard_map(
        chosen,
        mesh=mesh,
        in_specs=(
            P(("fs", "rep"), "tp"),
            P(("fs", "rep"), "tp"),
            P("tp"),
            P(),
            P(("fs", "rep"), None),
            P("tp", None),
            P("tp", "fs"),
            P("fs", "tp"),
            P("fs", "tp"),
        ),
        out_specs=(P("tp", "fs"), P("tp", None), P("tp", "fs"), P("fs", "tp"), P("fs", "tp")),
        check_vma=False,
    )
```
